256 devices in a mesh: ep: 64 (over z, y, core), tp: 4 (over x).
Axes of the slice: x: 4, y: 4, z: 8, core: 2. Of those that a mesh axis runs over, the one named last changes fastest.
Arguments:
- att_queries: bfloat16 [65536, 1024], P(('ep', 'tp')), may hold values from -8 to 8
- att_keys: bfloat16 [65536, 256], P(('ep', 'tp')), may hold values from -6 to 6
- att_values: bfloat16 [65536, 256], P(('ep', 'tp')), may hold values from -6 to 6
- sink_logits: float32 [16], replicated, may hold values from 3 to 6.5
- out_weight: bfloat16 [1024, 2048], replicated, may hold values from -0.1875 to 0.1875
- att_gain: float32 [2048], replicated, may hold values from 0.1 to 1.9
- moe_in: bfloat16 [32768, 2048], P(('ep', 'tp')), may hold values from -6 to 6
- pre_gain: float32 [2048], replicated, may hold values from 0.1 to 1.9
- expert_ids: int32 [32768, 2], P(('ep', 'tp')), may hold values from 0 to 127, all different within a row; in each aligned block of 128 rows (0 to 127, 128 to 255, ...) at most 4 rows name the same one
- routed_expert_weight: float32 [32768, 2], P(('ep', 'tp')), may hold values from 0.2 to 1.5
- w_gate: bfloat16 [128, 2048, 768], P('ep', None, 'tp'), may hold values from -0.125 to 0.125
- w_up: bfloat16 [128, 2048, 768], P('ep', None, 'tp'), may hold values from -0.125 to 0.125
- w_down: bfloat16 [128, 768, 2048], P('ep', 'tp'), may hold values from -0.21875 to 0.21875
- common_expert_gate_weight: bfloat16 [2048, 512], P(None, 'tp'), may hold values from -0.125 to 0.125
- common_expert_up_weight: bfloat16 [2048, 512], P(None, 'tp'), may hold values from -0.125 to 0.125
- common_expert_down_weight: bfloat16 [512, 2048], P('tp'), may hold values from -0.25 to 0.25
- moe_gain: float32 [2048], replicated, may hold values from 0.1 to 1.9
Outputs:
- mixer_out: bfloat16 [65536, 2048], P(('ep', 'tp'))
- experts_out: bfloat16 [32768, 2048], P(('ep', 'tp'))
The draws below stay inside these ranges and needn't reach their ends.
Inputs may be any that keep to these rules, and one draw needn't show every extreme that they name: `expert_ids`: each row names 2 different experts; within the rows of one device no expert is named more than 4 times, and in every draw some expert is named exactly 4 times by the rows of some device.
All inputs are finite; a program needn't handle non-finite values.
Results may differ from the reference program's by a relative error of at most 0.012.
Values may be sent and summed in bfloat16 or wider, within the bound.
No kernel may reach another device: no remote copies, remote signals or barrier semaphores. Data moves between devices by JAX's collectives and lax.ppermute only.
A program may use at most 128 MiB of HBM per device.

```python
import math
import jax
import jax.numpy as jnp
import numpy as np
from jax import lax

D = 2048
HEADS = 16
KV_HEADS = 4
HEAD_DIM = 64
WINDOW = 128
TOK_MOE = 128
TOPK = 2
FE = 768
SHARED = 512
EXPERTS = 128
CAP = 4
SEQ_ATT = 65536
TOKENS_MOE = 32768
N_EP = 64
N_TP = 4


def draw_att_queries(key, part):
    shape = (SEQ_ATT, KV_HEADS, HEADS // KV_HEADS, HEAD_DIM)
    base_draw = jax.random.truncated_normal(jax.random.fold_in(key, 21), -6.0, 6.0, shape, jnp.float32)
    return base_draw.reshape(SEQ_ATT, HEADS * HEAD_DIM).astype(jnp.bfloat16)


def draw_att_keys(key, part):
    shape = (SEQ_ATT, KV_HEADS, HEAD_DIM)
    base_draw = jax.random.truncated_normal(jax.random.fold_in(key, 31), -6.0, 6.0, shape, jnp.float32)
    return base_draw.reshape(SEQ_ATT, KV_HEADS * HEAD_DIM).astype(jnp.bfloat16)


def block_scale(stream_key, extent, cuts, least, largest):
    def one(dim, blocks):
        heights = jax.random.uniform(jax.random.fold_in(jax.random.fold_in(stream_key, 6), dim), (blocks,), jnp.float32, least / len(cuts), largest / len(cuts))
        return jnp.repeat(jnp.exp(heights), extent[dim] // blocks).reshape((-1,) + (1,) * (len(extent) - dim - 1))

    gain = one(*cuts[0])
    for cut in cuts[1:]:
        gain = gain * one(*cut)
    return gain


def deal_out(key, own, number, rows, amount, top, limit, lean):
    order = jax.random.permutation(key, amount)
    crowded, common = shares(amount, rows * top, limit, lean, True), shares(amount, rows * top, limit, lean, False)
    places = jnp.arange(amount)

    def named(tallies, rotation):
        used = int((tallies > 0).sum())
        fixed = max(1, used // 4)
        shifted = fixed + (places - fixed + rotation * (used - fixed)) % max(1, amount - fixed)
        return jnp.zeros((amount,), jnp.int32).at[order[jnp.where(places < fixed, places, shifted)]].set(jnp.asarray(tallies, jnp.int32))

    tallies = jnp.where(number % 4 == 0, named(crowded, number // 4), named(common, number - number // 4 - 1))
    mixed = jax.random.permutation(jax.random.fold_in(own, 3), amount)
    giver, taker = mixed[0:amount // 2 * 2:2], mixed[1:amount // 2 * 2:2]
    slack = jnp.minimum(tallies[giver] - 1, limit - tallies[taker]) // 2
    slack = jnp.where((giver == order[0]) | (taker == order[0]) | (tallies[taker] == 0), 0, jnp.maximum(slack, 0))
    shifted = jax.random.randint(jax.random.fold_in(own, 4), (amount // 2,), 0, 1 << 20) % (slack + 1)
    tallies = tallies.at[giver].add(-shifted).at[taker].add(shifted)
    members = jnp.searchsorted(jnp.cumsum(tallies), jnp.arange(rows * top), side="right").astype(jnp.int32)
    table = members.reshape(top, rows).T
    table = table[jax.random.permutation(jax.random.fold_in(own, 1), rows)]
    rotation = jax.random.randint(jax.random.fold_in(own, 2), (rows, 1), 0, top)
    return jnp.take_along_axis(table, (jnp.arange(top)[None, :] + rotation) % top, axis=1)


def shares(count, total, reach, lean, full):
    portions = [(1 << 20) // math.isqrt(rank ** lean) + 1 for rank in range(1, count + 1)]
    largest = reach if full else min(reach, max(-(-total // count), total * portions[0] // sum(portions)))
    least = 1 if total - largest >= count - 1 else 0
    given, rest = [largest] + [least] * (count - 1), total - largest - least * (count - 1)
    while rest > 0:
        free = [i for i in range(1, count) if given[i] < largest] or [i for i in range(1, count) if given[i] < reach]
        whole, budget = sum([portions[i] for i in free]), rest
        for i in free:
            more = min(reach - given[i], max(1, budget * portions[i] // whole), rest)
            given[i] = given[i] + more
            rest = rest - more
    return np.array(given)


def centred(stream_key, dims, width, reach, shards=(), kind=jnp.bfloat16):
    values = width * jax.random.normal(stream_key, dims, jnp.float32)
    if shards:
        values = values * block_scale(stream_key, dims, shards, -0.22, 0.18)
    return jnp.clip(values, -reach, reach).astype(kind)


def setup_inputs(seed: int = 0) -> dict:
    key_list = jax.random.split(jax.random.key(seed), 18)
    att_queries = draw_att_queries(jax.random.fold_in(key_list[17], 71), 0)
    att_keys = draw_att_keys(jax.random.fold_in(key_list[17], 71), 0)
    att_values = centred(key_list[2], (SEQ_ATT, KV_HEADS * HEAD_DIM), 1.0, 6.0, ((0, 256),))
    sink_logits = jnp.clip(jax.random.uniform(key_list[3], (HEADS,), jnp.float32, 3.0, 6.5), 3.0, 6.5)
    out_weight = centred(key_list[4], (HEADS * HEAD_DIM, D), (HEADS * HEAD_DIM) ** -0.5, 0.1875)
    att_gain = jnp.clip(1.0 + 0.18 * jax.random.normal(key_list[5], (D,), jnp.float32), 0.1, 1.9)
    moe_in = centred(key_list[6], (TOKENS_MOE, D), 1.0, 6.0, ((0, 256),))
    pre_gain = jnp.clip(1.0 + 0.18 * jax.random.normal(key_list[7], (D,), jnp.float32), 0.1, 1.9)
    expert_ids_keys = jax.random.split(jax.random.fold_in(key_list[8], 1), TOKENS_MOE // TOK_MOE)
    expert_ids_turns = jax.random.permutation(jax.random.fold_in(key_list[8], 3), TOKENS_MOE // TOK_MOE)
    expert_ids = jax.vmap(lambda own, number: deal_out(jax.random.fold_in(key_list[8], 2), own, number, TOK_MOE, EXPERTS, TOPK, CAP, 1))(expert_ids_keys, expert_ids_turns).reshape((TOKENS_MOE, TOPK))
    routed_expert_weight = jnp.clip(jnp.exp(math.log(1.5) - 2.014903 * jax.random.uniform(key_list[9], (TOKENS_MOE, TOPK), jnp.float32) ** block_scale(key_list[9], (TOKENS_MOE, TOPK), ((0, 256),), -0.2, 0.2)), 0.2, 1.5)
    w_gate = centred(key_list[10], (EXPERTS, D, FE), D ** -0.5, 0.125, ((0, 64), (2, 4)))
    w_up = centred(key_list[11], (EXPERTS, D, FE), D ** -0.5, 0.125, ((0, 64), (2, 4)))
    w_down = centred(key_list[12], (EXPERTS, FE, D), FE ** -0.5, 0.21875, ((0, 64), (1, 4)))
    common_expert_gate_weight = centred(key_list[13], (D, SHARED), D ** -0.5, 0.125, ((1, 4),))
    common_expert_up_weight = centred(key_list[14], (D, SHARED), D ** -0.5, 0.125, ((1, 4),))
    common_expert_down_weight = centred(key_list[15], (SHARED, D), SHARED ** -0.5, 0.25, ((0, 4),))
    moe_gain = jnp.clip(1.0 + 0.18 * jax.random.normal(key_list[16], (D,), jnp.float32), 0.1, 1.9)
    return {"att_queries": att_queries, "att_keys": att_keys, "att_values": att_values, "sink_logits": sink_logits, "out_weight": out_weight, "att_gain": att_gain, "moe_in": moe_in, "pre_gain": pre_gain, "expert_ids": expert_ids, "routed_expert_weight": routed_expert_weight, "w_gate": w_gate, "w_up": w_up, "w_down": w_down, "common_expert_gate_weight": common_expert_gate_weight, "common_expert_up_weight": common_expert_up_weight, "common_expert_down_weight": common_expert_down_weight, "moe_gain": moe_gain}


EPS = 1e-06
NEGATIVE = -1e+30

def rms_scale(inputs, gain_vec):
    mean_sq = lax.optimization_barrier(jnp.mean(inputs * inputs, axis=-1, keepdims=True))
    return inputs * lax.rsqrt(mean_sq + EPS) * gain_vec

def block_parts(hidden, down_rows, split_count):
    block_width = hidden.shape[-1] // split_count
    pieces = jnp.einsum('rbf,bfd->rbd', hidden.astype(jnp.float32).reshape(hidden.shape[0], split_count, block_width), down_rows.astype(jnp.float32).reshape(split_count, block_width, down_rows.shape[-1]))
    rounded = lax.optimization_barrier(pieces.astype(jnp.bfloat16))
    return lax.optimization_barrier(jnp.sum(rounded.astype(jnp.float32), axis=1))

def window_attention(att_queries, att_keys, att_values, sink_logits):
    group_size = HEADS // KV_HEADS
    blocks = SEQ_ATT // WINDOW
    padding = jnp.zeros((WINDOW, KV_HEADS * HEAD_DIM), att_keys.dtype)
    key_blocks = jnp.concatenate([padding, att_keys], axis=0).reshape(blocks + 1, WINDOW, KV_HEADS, HEAD_DIM)
    value_blocks = jnp.concatenate([padding, att_values], axis=0).reshape(blocks + 1, WINDOW, KV_HEADS, HEAD_DIM)
    query_blocks = att_queries.reshape(blocks, WINDOW, KV_HEADS, group_size, HEAD_DIM)
    distance = jnp.arange(WINDOW)[:, None] + WINDOW - jnp.arange(2 * WINDOW)[None, :]
    inside = (distance >= 0) & (distance < WINDOW)
    sink_grid = sink_logits.astype(jnp.float32).reshape(KV_HEADS, group_size)[:, :, None, None]
    score_scale = 1.0 / math.sqrt(HEAD_DIM)

    def one_block(block_index):
        key_band = lax.dynamic_slice_in_dim(key_blocks, block_index, 2, 0).reshape(2 * WINDOW, KV_HEADS, HEAD_DIM)
        value_band = lax.dynamic_slice_in_dim(value_blocks, block_index, 2, 0).reshape(2 * WINDOW, KV_HEADS, HEAD_DIM)
        query_block = lax.dynamic_index_in_dim(query_blocks, block_index, 0, keepdims=False)
        scores = jnp.einsum('qgjd,kgd->gjqk', query_block.astype(jnp.float32), key_band.astype(jnp.float32)) * score_scale
        key_pos = block_index * WINDOW - WINDOW + jnp.arange(2 * WINDOW)
        is_valid = inside & (key_pos >= 0)[None, :]
        scores = jnp.where(is_valid[None, None], scores, NEGATIVE)
        row_top = jnp.maximum(lax.optimization_barrier(jnp.max(scores, axis=-1, keepdims=True)), sink_grid)
        exp_scores = jnp.exp(scores - row_top)
        denominator = lax.optimization_barrier(jnp.sum(exp_scores, axis=-1, keepdims=True)) + jnp.exp(sink_grid - row_top)
        probs = (exp_scores / denominator).astype(jnp.bfloat16)
        head_mix = jnp.einsum('gjqk,kgd->qgjd', probs.astype(jnp.float32), value_band.astype(jnp.float32))
        return head_mix.astype(jnp.bfloat16).reshape(WINDOW, HEADS * HEAD_DIM)
    head_mix = lax.map(one_block, jnp.arange(blocks, dtype=jnp.int32))
    return head_mix.reshape(SEQ_ATT, HEADS * HEAD_DIM)

def routed_experts(normed, expert_ids, routed_expert_weight, w_gate, w_up, w_down):
    devices = N_EP * N_TP
    per_device = TOK_MOE * TOPK
    flat_ids = expert_ids.reshape(devices, per_device)
    earlier = jnp.arange(per_device)[None, :] < jnp.arange(per_device)[:, None]

    def positions_of(device_ids):
        return lax.optimization_barrier(jnp.sum((device_ids[:, None] == device_ids[None, :]) & earlier, axis=1)).astype(jnp.int32)
    position = lax.map(positions_of, flat_ids)
    device_index = jnp.arange(devices, dtype=jnp.int32)[:, None]
    slot_index = ((flat_ids * devices + device_index) * CAP + position).reshape(-1).astype(jnp.int32)
    token_index = (device_index * TOK_MOE + jnp.arange(per_device, dtype=jnp.int32)[None, :] // TOPK).reshape(-1)
    table_size = EXPERTS * devices * CAP
    row_table = jnp.zeros((table_size,), jnp.int32).at[slot_index].set(token_index.astype(jnp.int32))
    row_table = row_table.reshape(EXPERTS, devices * CAP)
    weight_table = jnp.zeros((table_size,), jnp.float32).at[slot_index].set(routed_expert_weight.reshape(-1))
    weight_table = weight_table.reshape(EXPERTS, devices * CAP)

    def add_expert(running, expert_index):
        row_ids = lax.dynamic_index_in_dim(row_table, expert_index, 0, keepdims=False)
        slot_weights = lax.dynamic_index_in_dim(weight_table, expert_index, 0, keepdims=False)
        picked = normed[row_ids]
        gate_act = jnp.dot(picked, w_gate[expert_index], preferred_element_type=jnp.float32)
        up_act = jnp.dot(picked, w_up[expert_index], preferred_element_type=jnp.float32)
        hidden = (jax.nn.silu(gate_act) * up_act).astype(jnp.bfloat16)
        output = block_parts(hidden, w_down[expert_index], N_TP).astype(jnp.bfloat16)
        running = running.at[row_ids].add(slot_weights[:, None] * output.astype(jnp.float32))
        return (running, None)
    start_value = jnp.zeros((TOKENS_MOE, D), jnp.float32)
    return lax.scan(add_expert, start_value, jnp.arange(EXPERTS, dtype=jnp.int32))[0]

def reference(att_queries, att_keys, att_values, sink_logits, out_weight, att_gain, moe_in, pre_gain, expert_ids, routed_expert_weight, w_gate, w_up, w_down, common_expert_gate_weight, common_expert_up_weight, common_expert_down_weight, moe_gain):
    head_mix = window_attention(att_queries, att_keys, att_values, sink_logits)
    projected = jnp.dot(head_mix, out_weight, preferred_element_type=jnp.float32)
    mixer_out = rms_scale(projected, att_gain).astype(jnp.bfloat16)
    normed = rms_scale(moe_in.astype(jnp.float32), pre_gain).astype(jnp.bfloat16)
    routed = routed_experts(normed, expert_ids, routed_expert_weight, w_gate, w_up, w_down)

    def shared_rows(row_block):
        gate_act = jnp.dot(row_block, common_expert_gate_weight, preferred_element_type=jnp.float32)
        up_act = jnp.dot(row_block, common_expert_up_weight, preferred_element_type=jnp.float32)
        common_expert_hidden = (jax.nn.silu(gate_act) * up_act).astype(jnp.bfloat16)
        return block_parts(common_expert_hidden, common_expert_down_weight, N_TP)
    shared_sum = lax.map(shared_rows, normed.reshape(N_EP * N_TP, TOK_MOE, D)).reshape(TOKENS_MOE, D)
    combined = routed + shared_sum
    experts_out = rms_scale(combined, moe_gain).astype(jnp.bfloat16)
    return (mixer_out, experts_out)
```

```python
import math

import jax
import jax.numpy as jnp
from jax import lax
from jax.experimental import pallas as pl
from jax.experimental.pallas import tpu as pltpu
from jax.sharding import Mesh
from jax.sharding import PartitionSpec as P


HEADS = 16
KV_HEADS = 4
HEAD_DIM = 64
WINDOW = 128
CAP = 4
BLOCK = 256
EP = ("z", "y", "c")
EP_TP = ("z", "y", "c", "tp")
CHIPS = ("z", "y", "tp")
CORE_TP = ("c", "tp")
EPS = 1e-06
NEGATIVE = -1e30


f32 = jnp.float32
bf16 = jnp.bfloat16
VMEM = pltpu.VMEM
ANY = pl.ANY


def iota(shape, dim):
    return lax.broadcasted_iota(jnp.int32, shape, dim)


def dot(a, b):
    return jnp.dot(a, b, preferred_element_type=f32)


def dot_t(a, b):
    return lax.dot_general(a, b, (((1,), (1,)), ((), ())), preferred_element_type=f32)


def in_vmem(count):
    return [pl.BlockSpec(memory_space=VMEM)] * count


def from_behind(block, axis, distance):
    devices = range(lax.axis_size(axis))
    route = [(i - distance, i) for i in devices if i - distance in devices]
    return lax.ppermute(block, axis, route)


def rms_scale(inputs, gain_vec):
    mean_sq = jnp.mean(inputs * inputs, axis=-1, keepdims=True)
    return inputs * lax.rsqrt(mean_sq + EPS) * gain_vec


def slot_rows(ids, lanes):
    tokens = ids.shape[1]
    shape = (tokens, tokens)
    eye = iota(shape, 0) == iota(shape, 1)
    across = [ids[k : k + 1, :] for k in range(2)]
    down = [jnp.sum(jnp.where(eye, a, 0.0), axis=1, keepdims=True) for a in across]
    if lanes:
        mine, theirs, axis, earlier = across, down, 0, iota(shape, 0) < iota(shape, 1)
    else:
        mine, theirs, axis, earlier = down, across, 1, iota(shape, 1) < iota(shape, 0)
    rows = []
    for k in range(2):
        place = sum(
            jnp.sum(jnp.where((mine[k] == other) & earlier, 1.0, 0.0), axis=axis, keepdims=True)
            for other in theirs
        )
        rows.append((mine[k] * (2 * CAP) + place).astype(jnp.int32))
    return rows


def pack_kernel(x_ref, gain_ref, ids_ref, packed_ref, normed_ref, stacked):
    half = x_ref.shape[1] // 2
    tokens = x_ref.shape[0]
    step = pl.program_id(0)
    block = packed_ref.shape[0]

    @pl.when(step == 0)
    def _():
        x = x_ref[...].astype(f32)
        normed = rms_scale(x, gain_ref[...]).astype(bf16)
        normed_ref[...] = normed
        stacked[:tokens, :] = normed[:, :half]
        stacked[tokens:, :] = normed[:, half:]

    rows = slot_rows(ids_ref[...].astype(f32), True)
    r = iota((block, tokens), 0) + step * block
    chosen = jnp.concatenate(
        [
            jnp.where((r == rows[0] + h * CAP) | (r == rows[1] + h * CAP), 1.0, 0.0).astype(bf16)
            for h in range(2)
        ],
        axis=1,
    )
    packed_ref[...] = dot(chosen, stacked[...]).astype(bf16)


def pack(x, gain, ids, slots):
    tokens, width = x.shape
    steps = 4
    total = 2 * slots
    return pl.pallas_call(
        pack_kernel,
        grid=(steps,),
        in_specs=[
            pl.BlockSpec((tokens, width), lambda i: (0, 0)),
            pl.BlockSpec((1, width), lambda i: (0, 0)),
            pl.BlockSpec((2, tokens), lambda i: (0, 0)),
        ],
        out_specs=[
            pl.BlockSpec((total // steps, width // 2), lambda i: (i, 0)),
            pl.BlockSpec((tokens, width), lambda i: (0, 0)),
        ],
        out_shape=[
            jax.ShapeDtypeStruct((total, width // 2), bf16),
            jax.ShapeDtypeStruct((tokens, width), bf16),
        ],
        scratch_shapes=[VMEM((2 * tokens, width // 2), bf16)],
        cost_estimate=pl.CostEstimate(
            flops=2 * total * tokens * width, bytes_accessed=6 * tokens * width, transcendentals=0
        ),
        name="pack",
    )(x, gain, ids)


def expert_kernel(own_ref, recv, *refs):
    own, other = refs[:4], refs[4:8]
    out_ref, arrived, gate, up, down, rows, hidden, sem, sems = refs[8:]
    part = own[0].shape[0] // 3
    half = recv.shape[1]
    groups = recv.shape[0] // BLOCK

    def fill(k, m, piece):
        into = (gate, up, down)[m]
        return pltpu.make_async_copy(
            piece.at[pl.ds(m * part, part)], into.at[pl.ds(k * part, part)], sems.at[m, k]
        )

    rows_in = pltpu.make_async_copy(recv, arrived, sem)
    rows_in.start()
    for mine, pieces in ((1, own), (0, other)):

        @pl.when(own_ref[0] == mine)
        def _():
            for m in range(3):
                for k, piece in enumerate(pieces):
                    fill(k, m, piece).start()

    def wait(m):
        for k in range(4):
            fill(k, m, own[k]).wait()

    a, b = iota((BLOCK // 2, BLOCK), 0), iota((BLOCK // 2, BLOCK), 1)
    first = (a // CAP) * (2 * CAP) + a % CAP
    picks = [jnp.where(b == first + h * CAP, 1.0, 0.0).astype(bf16) for h in range(2)]
    rows_in.wait()

    def sort_rows(i, carry):
        block = arrived[pl.ds(pl.multiple_of(i * BLOCK, BLOCK), BLOCK), :]
        at = pl.ds(pl.multiple_of(i * (BLOCK // 2), BLOCK // 2), BLOCK // 2)
        for h in range(2):
            rows[at, h * half : (h + 1) * half] = dot(picks[h], block).astype(bf16)
        return carry

    lax.fori_loop(0, groups, sort_rows, 0)
    wait(0)
    wait(1)

    def units(n, carry):
        at = pl.ds(pl.multiple_of(n * BLOCK, BLOCK), BLOCK)
        x = rows[...]
        g = dot_t(x, gate[at, :])
        u = dot_t(x, up[at, :])
        hidden[:, at] = (g / (1.0 + jnp.exp(-g)) * u).astype(bf16)
        return carry

    lax.fori_loop(0, hidden.shape[1] // BLOCK, units, 0)
    wait(2)
    a, b = iota((BLOCK, BLOCK), 0), iota((BLOCK, BLOCK), 1)
    b, h = b % (BLOCK // 2), b // (BLOCK // 2)
    back = jnp.where(a == (b // CAP) * (2 * CAP) + b % CAP + h * CAP, 1.0, 0.0).astype(bf16)

    def columns(n, carry):
        at = pl.multiple_of(n * BLOCK, BLOCK)
        x = hidden[...]
        left = dot(x, down[:, pl.ds(at, BLOCK)]).astype(bf16)
        right = dot(x, down[:, pl.ds(half + at, BLOCK)]).astype(bf16)
        for i in range(groups):
            mine = slice(i * (BLOCK // 2), (i + 1) * (BLOCK // 2))
            both = jnp.concatenate([left[mine], right[mine]], axis=0)
            out_ref[i * BLOCK : (i + 1) * BLOCK, pl.ds(at, BLOCK)] = dot(back, both).astype(bf16)
        return carry

    lax.fori_loop(0, half // BLOCK, columns, 0)


def expert(own, recv, mine, others):
    total, half = recv.shape
    units = 4 * mine[0].shape[0] // 3
    return pl.pallas_call(
        expert_kernel,
        in_specs=[pl.BlockSpec(memory_space=pltpu.SMEM)] + [pl.BlockSpec(memory_space=ANY)] * 9,
        out_specs=pl.BlockSpec(memory_space=VMEM),
        out_shape=jax.ShapeDtypeStruct((total, half), bf16),
        scratch_shapes=[
            VMEM((total, half), bf16),
            VMEM((units, 2 * half), bf16),
            VMEM((units, 2 * half), bf16),
            VMEM((units, 2 * half), bf16),
            VMEM((total // 2, 2 * half), bf16),
            VMEM((total // 2, units), bf16),
            pltpu.SemaphoreType.DMA,
            pltpu.SemaphoreType.DMA((3, 4)),
        ],
        cost_estimate=pl.CostEstimate(
            flops=6 * total * half * units,
            bytes_accessed=4 * total * half + 12 * half * units,
            transcendentals=total * units // 2,
        ),
        name="expert",
    )(own, recv, *mine, *others)


def shared_prep_kernel(core_ref, gate_ref, up_ref, down_ref, out_ref):
    depth = gate_ref.shape[0] // 2
    units = gate_ref.shape[1]
    core = core_ref[0]
    at = pl.ds(pl.multiple_of(core * depth, depth), depth)
    out_ref[:depth, :] = gate_ref[at, :]
    out_ref[depth : 2 * depth, :] = up_ref[at, :]
    for t in range(depth // 128):
        lane = pl.multiple_of(core * depth + t * 128, 128)
        out_ref[2 * depth + t * units : 2 * depth + (t + 1) * units, :] = down_ref[
            :, pl.ds(lane, 128)
        ]


def shared_prep(core, gate, up, down):
    return pl.pallas_call(
        shared_prep_kernel,
        in_specs=[pl.BlockSpec(memory_space=pltpu.SMEM)] + in_vmem(3),
        out_specs=pl.BlockSpec(memory_space=VMEM),
        out_shape=jax.ShapeDtypeStruct((gate.shape[0] // 2 * 3, gate.shape[1]), bf16),
        cost_estimate=pl.CostEstimate(flops=1000, bytes_accessed=12 * gate.size, transcendentals=0),
        name="shared_prep",
    )(core, gate, up, down)


def shared_kernel(core_ref, x_ref, *refs):
    mine, theirs = refs[:4], refs[4:8]
    out_ref, into, down = refs[8:]
    depth = x_ref.shape[1] // 2
    units = mine[0].shape[1]
    core = core_ref[0]
    for side, pieces in ((core, mine), (1 - core, theirs)):
        top = pl.multiple_of(side * depth, depth)
        for k, piece in enumerate(pieces):
            for m in range(2):
                lane = (m * 4 + k) * units
                into[pl.ds(top, depth), lane : lane + units] = piece[m * depth : (m + 1) * depth, :]
            for t in range(depth // 128):
                lane = pl.multiple_of(side * depth + t * 128, 128)
                at = 2 * depth + t * units
                down[k * units : (k + 1) * units, pl.ds(lane, 128)] = piece[at : at + units, :]
    both = dot(x_ref[...], into[...])
    g, u = both[:, : 4 * units], both[:, 4 * units :]
    hidden = (g / (1.0 + jnp.exp(-g)) * u).astype(bf16)
    out_ref[...] = dot(hidden, down[...])


def shared_expert(core, normed, mine, theirs):
    tokens, width = normed.shape
    units = 4 * mine[0].shape[1]
    return pl.pallas_call(
        shared_kernel,
        in_specs=[pl.BlockSpec(memory_space=pltpu.SMEM)] + in_vmem(9),
        out_specs=pl.BlockSpec(memory_space=VMEM),
        out_shape=jax.ShapeDtypeStruct((tokens, width), f32),
        scratch_shapes=[VMEM((width, 2 * units), bf16), VMEM((units, width), bf16)],
        cost_estimate=pl.CostEstimate(
            flops=6 * tokens * width * units,
            bytes_accessed=6 * width * units,
            transcendentals=tokens * units,
        ),
        name="shared_expert",
    )(core, normed, *mine, *theirs)


def combine_kernel(back_ref, ids_ref, weight_ref, shared_ref, gain_ref, out_ref):
    tokens = out_ref.shape[0]
    slots, half = back_ref.shape
    first = slot_rows(ids_ref[...].astype(f32), False)
    eye = iota((tokens, tokens), 0) == iota((tokens, tokens), 1)
    weights = [
        jnp.sum(jnp.where(eye, weight_ref[k : k + 1, :], 0.0), axis=1, keepdims=True)
        for k in range(2)
    ]
    r = iota((tokens, slots), 1)
    back = back_ref[...]
    halves = []
    for h in range(2):
        spread = jnp.where(r == first[0] + h * CAP, weights[0], 0.0) + jnp.where(
            r == first[1] + h * CAP, weights[1], 0.0
        )
        coarse = spread.astype(bf16)
        fine = (spread - coarse.astype(f32)).astype(bf16)
        summed = dot(jnp.concatenate([coarse, fine], axis=0), back)
        halves.append(
            summed[:tokens] + summed[tokens:] + shared_ref[:, h * half : (h + 1) * half]
        )
    square = sum(jnp.sum(v * v, axis=1, keepdims=True) for v in halves)
    scale = lax.rsqrt(square / (2 * half) + EPS)
    for h, v in enumerate(halves):
        at = slice(h * half, (h + 1) * half)
        out_ref[:, at] = (v * scale * gain_ref[:, at]).astype(bf16)


def combine(back, ids, weights, shared, gain):
    slots, half = back.shape
    tokens = ids.shape[1]
    return pl.pallas_call(
        combine_kernel,
        in_specs=in_vmem(5),
        out_specs=pl.BlockSpec(memory_space=VMEM),
        out_shape=jax.ShapeDtypeStruct((tokens, 2 * half), bf16),
        cost_estimate=pl.CostEstimate(
            flops=8 * tokens * slots * half, bytes_accessed=2 * slots * half, transcendentals=0
        ),
        name="combine",
    )(back, ids, weights, shared, gain)


def attention_kernel(
    first_ref, sink_ref, q_ref, k_ref, v_ref, rim_ref, weight_ref, gain_ref, out_ref, keys, values, mix, wide
):
    tokens = q_ref.shape[0]
    lanes = 2 * HEAD_DIM
    group = HEADS // KV_HEADS
    tiles = k_ref.shape[1] // lanes
    for into, rim, own in ((keys, 0, k_ref), (values, 1, v_ref)):
        for t in range(tiles):
            at = slice(t * lanes, (t + 1) * lanes)
            rows = jnp.concatenate([rim_ref[rim, :, at], own[:, at]], axis=0)
            into[2 * t] = rows
            into[2 * t + 1] = jnp.concatenate([rows[:, HEAD_DIM:], rows[:, :HEAD_DIM]], axis=1)
    i, j = iota((WINDOW, 2 * WINDOW), 0), iota((WINDOW, 2 * WINDOW), 1)
    low = iota((WINDOW, lanes), 1) < HEAD_DIM

    for n in range(tokens // WINDOW):
        band = slice(n * WINDOW, (n + 2) * WINDOW)
        at = slice(n * WINDOW, (n + 1) * WINDOW)
        inside = (j > i) & (j <= i + WINDOW)
        if n == 0:
            inside = inside & (j >= first_ref[0] * WINDOW)
        for g in range(KV_HEADS):
            kt = [2 * (g // 2) + (g + s) % 2 for s in range(2)]
            for t in range(group // 2):
                tile = g * (group // 2) + t
                q = q_ref[at, tile * lanes : (tile + 1) * lanes]
                mixed = []
                for s in range(2):
                    mine = jnp.where(low if s == 0 else ~low, q, jnp.zeros_like(q))
                    score = dot_t(mine, keys[kt[s], band, :]) * (1.0 / math.sqrt(HEAD_DIM))
                    score = jnp.where(inside, score, NEGATIVE)
                    sink = sink_ref[2 * tile + s]
                    top = jnp.maximum(jnp.max(score, axis=1, keepdims=True), sink)
                    e = jnp.exp(score - top)
                    below = jnp.sum(e, axis=1, keepdims=True) + jnp.exp(sink - top)
                    mixed.append(dot((e / below).astype(bf16), values[kt[s], band, :]))
                mix[at, tile * lanes : (tile + 1) * lanes] = jnp.where(
                    low, mixed[0], mixed[1]
                ).astype(bf16)

    width = 512
    square = jnp.zeros((tokens, 1), f32)
    for n in range(out_ref.shape[1] // width):
        at = slice(n * width, (n + 1) * width)
        p = dot(mix[...], weight_ref[:, at])
        wide[:, at] = p
        square = square + jnp.sum(p * p, axis=1, keepdims=True)
    scale = lax.rsqrt(square / out_ref.shape[1] + EPS)
    for n in range(out_ref.shape[1] // width):
        at = slice(n * width, (n + 1) * width)
        out_ref[:, at] = (wide[:, at] * scale * gain_ref[:, at]).astype(bf16)


def attention(first, sinks, queries, keys, values, rim, weight, gain):
    tokens, wide = queries.shape[0], weight.shape[1]
    lanes = 2 * HEAD_DIM
    rows = tokens + WINDOW
    return pl.pallas_call(
        attention_kernel,
        in_specs=[pl.BlockSpec(memory_space=pltpu.SMEM)] * 2 + in_vmem(6),
        out_specs=pl.BlockSpec(memory_space=VMEM),
        out_shape=jax.ShapeDtypeStruct((tokens, wide), bf16),
        scratch_shapes=[
            VMEM((KV_HEADS, rows, lanes), bf16),
            VMEM((KV_HEADS, rows, lanes), bf16),
            VMEM((tokens, HEADS * HEAD_DIM), bf16),
            VMEM((tokens, wide), f32),
        ],
        cost_estimate=pl.CostEstimate(
            flops=2 * tokens * HEADS * HEAD_DIM * (wide + 8 * WINDOW),
            bytes_accessed=2 * weight.size + 4 * tokens * wide,
            transcendentals=tokens * HEADS * 2 * WINDOW,
        ),
        name="attention",
    )(first, sinks, queries, keys, values, rim, weight, gain)


def body(
    att_queries,
    att_keys,
    att_values,
    sink_logits,
    out_weight,
    att_gain,
    moe_in,
    pre_gain,
    expert_ids,
    routed_expert_weight,
    w_gate,
    w_up,
    w_down,
    common_expert_gate_weight,
    common_expert_up_weight,
    common_expert_down_weight,
    moe_gain,
):
    x, core = lax.axis_index("tp"), lax.axis_index("c")
    tp = lax.axis_size("tp")
    homes = [(i // 2, i) for i in range(tp)]
    to_home = {
        k: [(c * tp + (i - k) % tp, c * tp + i) for c, i in homes] for k in range(1, tp)
    }
    to_other = [(c * tp + i, (1 - c) * tp + i) for c, i in homes]
    own = (core == x // 2).astype(jnp.int32).reshape(1)
    core_at = core.astype(jnp.int32).reshape(1)

    kv_rows = jnp.stack([att_keys, att_values])
    rim_rows = from_behind(kv_rows[:, att_keys.shape[0] - WINDOW :], EP_TP, 1)
    first = (lax.axis_index(EP_TP) == 0).astype(jnp.int32).reshape(1)

    gate_t, up_t = w_gate.transpose(0, 2, 1), w_up.transpose(0, 2, 1)

    def expert_of(parity, arrays):
        j = (x + parity) % 2
        return jnp.concatenate(
            [lax.dynamic_index_in_dim(a, j, 0, keepdims=False) for a in arrays], axis=0
        )

    def homeward(k, piece):
        return lax.ppermute(piece, CORE_TP, to_home[k])

    def across(pieces):
        return [lax.ppermute(v, CORE_TP, to_other) for v in pieces]

    pieces = {p: expert_of(p, (gate_t, up_t, w_down)) for p in (1, 0)}
    mine = [pieces[0]] + [homeward(k, pieces[k % 2]) for k in (1, 3, 2)]
    mine[2], mine[3] = mine[3], mine[2]
    others = across(mine)

    ids_t = expert_ids.T
    packed, normed = pack(moe_in, pre_gain.reshape(1, -1), ids_t, 128 * CAP)
    chips = packed.shape[0] // (2 * CAP)
    arrived = lax.all_to_all(
        packed.reshape(chips, 2 * CAP, -1), CHIPS, split_axis=0, concat_axis=0, tiled=True
    ).reshape(packed.shape)

    mixer_out = attention(
        first,
        sink_logits,
        att_queries,
        att_keys,
        att_values,
        rim_rows,
        out_weight,
        att_gain.reshape(1, -1),
    )

    out = expert(own, arrived, mine, others)
    returned = lax.all_to_all(
        out.reshape(chips, 2 * CAP, -1), CHIPS, split_axis=0, concat_axis=0, tiled=True
    ).reshape(out.shape)

    prepared = shared_prep(
        core_at,
        common_expert_gate_weight,
        common_expert_up_weight,
        common_expert_down_weight,
    )
    blocks = [prepared]
    for k in range(1, tp):
        blocks.append(lax.ppermute(prepared, "tp", [(i, (i + k) % tp) for i in range(tp)]))
    theirs = [lax.ppermute(v, "c", [(0, 1), (1, 0)]) for v in blocks]
    shared_sum = shared_expert(core_at, normed, blocks, theirs)
    experts_out = combine(
        returned, ids_t, routed_expert_weight.T, shared_sum, moe_gain.reshape(1, -1)
    )
    return (mixer_out, experts_out)


def solution(mesh):
    split = Mesh(mesh.devices.reshape(8, 4, 2, mesh.shape["tp"]), ("z", "y", "c", "tp"))
    placed = (
        P(EP_TP, None),
        P(EP_TP, None),
        P(EP_TP, None),
        P(),
        P(),
        P(),
        P(EP_TP, None),
        P(),
        P(EP_TP, None),
        P(EP_TP, None),
        P(EP, None, "tp"),
        P(EP, None, "tp"),
        P(EP, "tp", None),
        P(None, "tp"),
        P(None, "tp"),
        P("tp", None),
        P(),
    )
    return jax.shard_map(
        body,
        mesh=split,
        in_specs=placed,
        out_specs=(P(EP_TP, None), P(EP_TP, None)),
        check_vma=False,
    )
```

```python
import math

import jax
import jax.numpy as jnp
from jax import lax
from jax.experimental import pallas as pl
from jax.experimental.pallas import tpu as pltpu
from jax.sharding import Mesh
from jax.sharding import PartitionSpec as P


HEADS = 16
KV_HEADS = 4
HEAD_DIM = 64
WINDOW = 128
CAP = 4
BLOCK = 256
MIB = 1 << 20
PARTS = 4
COMBINE_LIMIT = 16
UP_LIMIT = 24
DOWN_LIMIT = 16
EP = ("z", "y", "c")
EP_TP = ("z", "y", "c", "tp")
CHIPS = ("z", "y", "tp")
CORE_TP = ("c", "tp")
EPS = 1e-06
NEGATIVE = -1e30


f32 = jnp.float32
bf16 = jnp.bfloat16
VMEM = pltpu.VMEM
ANY = pl.ANY


def iota(shape, dim):
    return lax.broadcasted_iota(jnp.int32, shape, dim)


def dot(a, b):
    return jnp.dot(a, b, preferred_element_type=f32)


def dot_t(a, b):
    return lax.dot_general(a, b, (((1,), (1,)), ((), ())), preferred_element_type=f32)


def in_vmem(count):
    return [pl.BlockSpec(memory_space=VMEM)] * count


def from_behind(block, axis, distance):
    devices = range(lax.axis_size(axis))
    route = [(i - distance, i) for i in devices if i - distance in devices]
    return lax.ppermute(block, axis, route)


def rms_scale(inputs, gain_vec):
    mean_sq = jnp.mean(inputs * inputs, axis=-1, keepdims=True)
    return inputs * lax.rsqrt(mean_sq + EPS) * gain_vec


def slot_rows(ids, lanes):
    tokens = ids.shape[1]
    shape = (tokens, tokens)
    eye = iota(shape, 0) == iota(shape, 1)
    across = [ids[k : k + 1, :] for k in range(2)]
    down = [jnp.sum(jnp.where(eye, a, 0.0), axis=1, keepdims=True) for a in across]
    if lanes:
        mine, theirs, axis, earlier = across, down, 0, iota(shape, 0) < iota(shape, 1)
    else:
        mine, theirs, axis, earlier = down, across, 1, iota(shape, 1) < iota(shape, 0)
    rows = []
    for k in range(2):
        place = sum(
            jnp.sum(jnp.where((mine[k] == other) & earlier, 1.0, 0.0), axis=axis, keepdims=True)
            for other in theirs
        )
        rows.append((mine[k] * (2 * CAP) + place).astype(jnp.int32))
    return rows


def pack_kernel(x_ref, gain_ref, ids_ref, packed_ref, normed_ref, stacked):
    half = x_ref.shape[1] // 2
    tokens = x_ref.shape[0]
    step = pl.program_id(0)
    block = packed_ref.shape[0]

    @pl.when(step == 0)
    def _():
        x = x_ref[...].astype(f32)
        normed = rms_scale(x, gain_ref[...]).astype(bf16)
        normed_ref[...] = normed
        stacked[:tokens, :] = normed[:, :half]
        stacked[tokens:, :] = normed[:, half:]

    rows = slot_rows(ids_ref[...].astype(f32), True)
    r = iota((block, tokens), 0) + step * block
    chosen = jnp.concatenate(
        [
            jnp.where((r == rows[0] + h * CAP) | (r == rows[1] + h * CAP), 1.0, 0.0).astype(bf16)
            for h in range(2)
        ],
        axis=1,
    )
    packed_ref[...] = dot(chosen, stacked[...]).astype(bf16)


def pack(x, gain, ids, slots):
    tokens, width = x.shape
    steps = 4
    total = 2 * slots
    return pl.pallas_call(
        pack_kernel,
        grid=(steps,),
        in_specs=[
            pl.BlockSpec((tokens, width), lambda i: (0, 0)),
            pl.BlockSpec((1, width), lambda i: (0, 0)),
            pl.BlockSpec((2, tokens), lambda i: (0, 0)),
        ],
        out_specs=[
            pl.BlockSpec((total // steps, width // 2), lambda i: (i, 0)),
            pl.BlockSpec((tokens, width), lambda i: (0, 0)),
        ],
        out_shape=[
            jax.ShapeDtypeStruct((total, width // 2), bf16),
            jax.ShapeDtypeStruct((tokens, width), bf16),
        ],
        scratch_shapes=[VMEM((2 * tokens, width // 2), bf16)],
        cost_estimate=pl.CostEstimate(
            flops=2 * total * tokens * width, bytes_accessed=6 * tokens * width, transcendentals=0
        ),
        name="pack",
    )(x, gain, ids)


def pick_kernel(parity_ref, *refs):
    arrays, outs, held, sems = refs[:-4], refs[-4:-2], refs[-2], refs[-1]
    rows = arrays[0].shape[1]
    steps = []
    for p, out in enumerate(outs):
        j = lax.rem(parity_ref[0] + p, 2)
        for m, array in enumerate(arrays):
            at = pl.ds(m * rows, rows)
            steps.append(
                (
                    pltpu.make_async_copy(array.at[j], held.at[p, at], sems.at[0, p, m]),
                    pltpu.make_async_copy(held.at[p, at], out.at[at], sems.at[1, p, m]),
                )
            )
    for c, _ in steps:
        c.start()
    for c, d in steps:
        c.wait()
        d.start()
    for _, d in steps:
        d.wait()


def pick(parity, arrays, limit):
    rows, width = arrays[0].shape[1:]
    count = len(arrays)
    return pl.pallas_call(
        pick_kernel,
        in_specs=[pl.BlockSpec(memory_space=pltpu.SMEM)] + [pl.BlockSpec(memory_space=ANY)] * count,
        out_specs=[pl.BlockSpec(memory_space=ANY)] * 2,
        out_shape=[jax.ShapeDtypeStruct((count * rows, width), bf16)] * 2,
        scratch_shapes=[
            VMEM((2, count * rows, width), bf16),
            pltpu.SemaphoreType.DMA((2, 2, count)),
        ],
        compiler_params=pltpu.CompilerParams(vmem_limit_bytes=limit * MIB),
        cost_estimate=pl.CostEstimate(
            flops=1000, bytes_accessed=8 * count * rows * width, transcendentals=0
        ),
        name="pick",
    )(parity, *arrays)


def start_pieces(own_ref, own, other, copy, parts):
    for mine, pieces in ((1, own), (0, other)):

        @pl.when(own_ref[0] == mine)
        def _():
            for m in range(parts):
                for k, piece in enumerate(pieces):
                    copy(k, m, piece).start()


def up_kernel(own_ref, recv, *refs):
    own, other = refs[:4], refs[4:8]
    hidden_ref, arrived, gate, up, rows, sem, sems = refs[8:]
    part = own[0].shape[0] // 2
    half = recv.shape[1]

    def copy(k, m, piece):
        return pltpu.make_async_copy(
            piece.at[pl.ds(m * part, part)], (gate, up)[m].at[pl.ds(k * part, part)], sems.at[m, k]
        )

    rows_in = pltpu.make_async_copy(recv, arrived, sem)
    rows_in.start()
    start_pieces(own_ref, own, other, copy, 2)
    a, b = iota((BLOCK // 2, BLOCK), 0), iota((BLOCK // 2, BLOCK), 1)
    first = (a // CAP) * (2 * CAP) + a % CAP
    picks = [jnp.where(b == first + h * CAP, 1.0, 0.0).astype(bf16) for h in range(2)]
    rows_in.wait()

    def sort_rows(i, carry):
        block = arrived[pl.ds(pl.multiple_of(i * BLOCK, BLOCK), BLOCK), :]
        at = pl.ds(pl.multiple_of(i * (BLOCK // 2), BLOCK // 2), BLOCK // 2)
        for h in range(2):
            rows[at, h * half : (h + 1) * half] = dot(picks[h], block).astype(bf16)
        return carry

    lax.fori_loop(0, recv.shape[0] // BLOCK, sort_rows, 0)
    for m in range(2):
        for k in range(4):
            copy(k, m, own[k]).wait()

    def units(n, carry):
        at = pl.ds(pl.multiple_of(n * BLOCK, BLOCK), BLOCK)
        x = rows[...]
        g = dot_t(x, gate[at, :])
        u = dot_t(x, up[at, :])
        hidden_ref[:, at] = (g / (1.0 + jnp.exp(-g)) * u).astype(bf16)
        return carry

    lax.fori_loop(0, hidden_ref.shape[1] // BLOCK, units, 0)


def expert_up(own, recv, mine, others):
    total, half = recv.shape
    units = 2 * mine[0].shape[0]
    return pl.pallas_call(
        up_kernel,
        in_specs=[pl.BlockSpec(memory_space=pltpu.SMEM)] + [pl.BlockSpec(memory_space=ANY)] * 9,
        out_specs=pl.BlockSpec(memory_space=VMEM),
        out_shape=jax.ShapeDtypeStruct((total // 2, units), bf16),
        scratch_shapes=[
            VMEM((total, half), bf16),
            VMEM((units, 2 * half), bf16),
            VMEM((units, 2 * half), bf16),
            VMEM((total // 2, 2 * half), bf16),
            pltpu.SemaphoreType.DMA,
            pltpu.SemaphoreType.DMA((2, 4)),
        ],
        compiler_params=pltpu.CompilerParams(vmem_limit_bytes=UP_LIMIT * MIB),
        cost_estimate=pl.CostEstimate(
            flops=4 * total * half * units,
            bytes_accessed=2 * total * half + 8 * half * units,
            transcendentals=total * units // 2,
        ),
        name="expert_up",
    )(own, recv, *mine, *others)


def down_kernel(own_ref, hidden, *refs):
    own, other = refs[:4], refs[4:8]
    out_ref, down, made, sems, out_sems = refs[8:]
    part = own[0].shape[0]
    half = out_ref.shape[1]
    groups = out_ref.shape[0] // BLOCK
    count = half // BLOCK

    def copies(n, pieces):
        return [
            pltpu.make_async_copy(
                piece.at[:, pl.ds(h * half + n * BLOCK, BLOCK)],
                down.at[pl.ds(k * part, part), pl.ds(h * half + n * BLOCK, BLOCK)],
                sems.at[n, h, k],
            )
            for h in range(2)
            for k, piece in enumerate(pieces)
        ]

    for mine, pieces in ((1, own), (0, other)):

        @pl.when(own_ref[0] == mine)
        def _():
            for n in range(count):
                for c in copies(n, pieces):
                    c.start()

    a, b = iota((BLOCK, BLOCK), 0), iota((BLOCK, BLOCK), 1)
    b, h = b % (BLOCK // 2), b // (BLOCK // 2)
    back = jnp.where(a == (b // CAP) * (2 * CAP) + b % CAP + h * CAP, 1.0, 0.0).astype(bf16)
    for n in range(count):
        for c in copies(n, own):
            c.wait()
        at = n * BLOCK
        x = hidden[...]
        left = dot(x, down[:, at : at + BLOCK]).astype(bf16)
        right = dot(x, down[:, half + at : half + at + BLOCK]).astype(bf16)
        for i in range(groups):
            mine = slice(i * (BLOCK // 2), (i + 1) * (BLOCK // 2))
            both = jnp.concatenate([left[mine], right[mine]], axis=0)
            made[i * BLOCK : (i + 1) * BLOCK, at : at + BLOCK] = dot(back, both).astype(bf16)
        columns = pl.ds(at, BLOCK)
        pltpu.make_async_copy(made.at[:, columns], out_ref.at[:, columns], out_sems.at[n]).start()
    for n in range(count):
        columns = pl.ds(n * BLOCK, BLOCK)
        pltpu.make_async_copy(made.at[:, columns], out_ref.at[:, columns], out_sems.at[n]).wait()


def expert_down(own, hidden, mine, others):
    rows, units = hidden.shape
    width = mine[0].shape[1]
    count = width // 2 // BLOCK
    return pl.pallas_call(
        down_kernel,
        in_specs=[pl.BlockSpec(memory_space=pltpu.SMEM)]
        + in_vmem(1)
        + [pl.BlockSpec(memory_space=ANY)] * 8,
        out_specs=pl.BlockSpec(memory_space=ANY),
        out_shape=jax.ShapeDtypeStruct((2 * rows, width // 2), bf16),
        scratch_shapes=[
            VMEM((units, width), bf16),
            VMEM((2 * rows, width // 2), bf16),
            pltpu.SemaphoreType.DMA((count, 2, 4)),
            pltpu.SemaphoreType.DMA((count,)),
        ],
        compiler_params=pltpu.CompilerParams(vmem_limit_bytes=DOWN_LIMIT * MIB),
        cost_estimate=pl.CostEstimate(
            flops=2 * rows * units * width,
            bytes_accessed=2 * (rows * (units + width) + units * width),
            transcendentals=0,
        ),
        name="expert_down",
    )(own, hidden, *mine, *others)


def shared_prep_kernel(part_ref, gate_ref, up_ref, down_ref, out_ref):
    depth = gate_ref.shape[0] // PARTS
    units = gate_ref.shape[1]
    first = pl.multiple_of(part_ref[0] * depth, depth)
    at = pl.ds(first, depth)
    out_ref[:depth, :] = gate_ref[at, :]
    out_ref[depth : 2 * depth, :] = up_ref[at, :]
    for t in range(depth // 128):
        lane = pl.multiple_of(first + t * 128, 128)
        out_ref[2 * depth + t * units : 2 * depth + (t + 1) * units, :] = down_ref[
            :, pl.ds(lane, 128)
        ]


def shared_prep(part, gate, up, down):
    return pl.pallas_call(
        shared_prep_kernel,
        in_specs=[pl.BlockSpec(memory_space=pltpu.SMEM)] + in_vmem(3),
        out_specs=pl.BlockSpec(memory_space=VMEM),
        out_shape=jax.ShapeDtypeStruct((gate.shape[0] // PARTS * 3, gate.shape[1]), bf16),
        compiler_params=pltpu.CompilerParams(vmem_limit_bytes=8 * MIB),
        cost_estimate=pl.CostEstimate(flops=1000, bytes_accessed=8 * gate.size, transcendentals=0),
        name="shared_prep",
    )(part, gate, up, down)


def slot_columns(ids, weights):
    tokens = ids.shape[1]
    first = slot_rows(ids.astype(f32), False)
    eye = iota((tokens, tokens), 0) == iota((tokens, tokens), 1)
    lane = iota((tokens, 128), 1)
    out = jnp.zeros((tokens, 128), f32)
    for k in range(2):
        weight = jnp.sum(jnp.where(eye, weights[k : k + 1, :], 0.0), axis=1, keepdims=True)
        out = jnp.where(lane == k, first[k].astype(f32), out)
        out = jnp.where(lane == 2 + k, weight, out)
    return out


def shared_kernel(part_ref, ids_ref, weight_ref, x_ref, *refs):
    parts, (out_ref, columns_ref, into, down) = refs[:PARTS], refs[PARTS:]
    depth = x_ref.shape[1] // PARTS
    units = parts[0].shape[1]
    for p, ref in enumerate(parts):
        first = pl.multiple_of(part_ref[p] * depth, depth)
        for k in range(4):
            base = 3 * k * depth
            for m in range(2):
                lane = (m * 4 + k) * units
                into[pl.ds(first, depth), lane : lane + units] = ref[
                    base + m * depth : base + (m + 1) * depth, :
                ]
            for t in range(depth // 128):
                lane = pl.multiple_of(first + t * 128, 128)
                at = base + 2 * depth + t * units
                down[k * units : (k + 1) * units, pl.ds(lane, 128)] = ref[at : at + units, :]
    both = dot(x_ref[...], into[...])
    g, u = both[:, : 4 * units], both[:, 4 * units :]
    hidden = (g / (1.0 + jnp.exp(-g)) * u).astype(bf16)
    out_ref[...] = dot(hidden, down[...])
    columns_ref[...] = slot_columns(ids_ref[...], weight_ref[...])


def shared_expert(part, ids, weights, normed, parts):
    tokens, width = normed.shape
    units = 4 * parts[0].shape[1]
    return pl.pallas_call(
        shared_kernel,
        in_specs=[pl.BlockSpec(memory_space=pltpu.SMEM)] + in_vmem(3 + PARTS),
        out_specs=[pl.BlockSpec(memory_space=VMEM)] * 2,
        out_shape=[
            jax.ShapeDtypeStruct((tokens, width), f32),
            jax.ShapeDtypeStruct((tokens, 128), f32),
        ],
        scratch_shapes=[VMEM((width, 2 * units), bf16), VMEM((units, width), bf16)],
        compiler_params=pltpu.CompilerParams(vmem_limit_bytes=24 * MIB),
        cost_estimate=pl.CostEstimate(
            flops=6 * tokens * width * units,
            bytes_accessed=6 * width * units,
            transcendentals=tokens * units,
        ),
        name="shared_expert",
    )(part, ids, weights, normed, *parts)


def combine_kernel(back_ref, shared_ref, columns_ref, gain_ref, out_ref, came, common, sems):
    tokens, half = out_ref.shape[0], back_ref.shape[1]
    back_in = pltpu.make_async_copy(back_ref, came, sems.at[0])
    shared_in = pltpu.make_async_copy(shared_ref, common, sems.at[1])
    back_in.start()
    shared_in.start()
    r = iota((tokens, back_ref.shape[0]), 1)
    first = [columns_ref[:, k : k + 1].astype(jnp.int32) for k in range(2)]
    weights = [columns_ref[:, 2 + k : 3 + k] for k in range(2)]
    spreads = []
    for h in range(2):
        spread = jnp.where(r == first[0] + h * CAP, weights[0], 0.0) + jnp.where(
            r == first[1] + h * CAP, weights[1], 0.0
        )
        coarse = spread.astype(bf16)
        fine = (spread - coarse.astype(f32)).astype(bf16)
        spreads += [coarse, fine]
    back_in.wait()
    summed = dot(jnp.concatenate(spreads, axis=0), came[...])
    shared_in.wait()
    halves = [
        summed[2 * h * tokens : (2 * h + 1) * tokens]
        + summed[(2 * h + 1) * tokens : (2 * h + 2) * tokens]
        + common[:, h * half : (h + 1) * half]
        for h in range(2)
    ]
    square = sum(jnp.sum(v * v, axis=1, keepdims=True) for v in halves)
    scale = lax.rsqrt(square / (2 * half) + EPS)
    for h, v in enumerate(halves):
        at = slice(h * half, (h + 1) * half)
        out_ref[:, at] = (v * scale * gain_ref[:, at]).astype(bf16)


def combine(back, shared, columns, gain):
    slots, half = back.shape
    tokens = shared.shape[0]
    return pl.pallas_call(
        combine_kernel,
        in_specs=[pl.BlockSpec(memory_space=ANY)] * 2 + in_vmem(2),
        out_specs=pl.BlockSpec(memory_space=VMEM),
        out_shape=jax.ShapeDtypeStruct((tokens, 2 * half), bf16),
        scratch_shapes=[
            VMEM((slots, half), bf16),
            VMEM((tokens, 2 * half), f32),
            pltpu.SemaphoreType.DMA((2,)),
        ],
        compiler_params=pltpu.CompilerParams(vmem_limit_bytes=COMBINE_LIMIT * MIB),
        cost_estimate=pl.CostEstimate(
            flops=8 * tokens * slots * half, bytes_accessed=2 * slots * half, transcendentals=0
        ),
        name="combine",
    )(back, shared, columns, gain)


def attention_kernel(
    first_ref, sink_ref, q_ref, k_ref, v_ref, rim_ref, weight_ref, gain_ref, out_ref, keys, values, mix, wide
):
    tokens = q_ref.shape[0]
    lanes = 2 * HEAD_DIM
    group = HEADS // KV_HEADS
    tiles = k_ref.shape[1] // lanes
    for into, rim, own in ((keys, 0, k_ref), (values, 1, v_ref)):
        for t in range(tiles):
            at = slice(t * lanes, (t + 1) * lanes)
            rows = jnp.concatenate([rim_ref[rim, :, at], own[:, at]], axis=0)
            into[2 * t] = rows
            into[2 * t + 1] = jnp.concatenate([rows[:, HEAD_DIM:], rows[:, :HEAD_DIM]], axis=1)
    i, j = iota((WINDOW, 2 * WINDOW), 0), iota((WINDOW, 2 * WINDOW), 1)
    low = iota((WINDOW, lanes), 1) < HEAD_DIM

    for n in range(tokens // WINDOW):
        band = slice(n * WINDOW, (n + 2) * WINDOW)
        at = slice(n * WINDOW, (n + 1) * WINDOW)
        inside = (j > i) & (j <= i + WINDOW)
        if n == 0:
            inside = inside & (j >= first_ref[0] * WINDOW)
        for g in range(KV_HEADS):
            kt = [2 * (g // 2) + (g + s) % 2 for s in range(2)]
            for t in range(group // 2):
                tile = g * (group // 2) + t
                q = q_ref[at, tile * lanes : (tile + 1) * lanes]
                mixed = []
                for s in range(2):
                    mine = jnp.where(low if s == 0 else ~low, q, jnp.zeros_like(q))
                    score = dot_t(mine, keys[kt[s], band, :]) * (1.0 / math.sqrt(HEAD_DIM))
                    score = jnp.where(inside, score, NEGATIVE)
                    sink = sink_ref[2 * tile + s]
                    top = jnp.maximum(jnp.max(score, axis=1, keepdims=True), sink)
                    e = jnp.exp(score - top)
                    below = jnp.sum(e, axis=1, keepdims=True) + jnp.exp(sink - top)
                    mixed.append(dot((e / below).astype(bf16), values[kt[s], band, :]))
                mix[at, tile * lanes : (tile + 1) * lanes] = jnp.where(
                    low, mixed[0], mixed[1]
                ).astype(bf16)

    width = 512
    square = jnp.zeros((tokens, 1), f32)
    for n in range(out_ref.shape[1] // width):
        at = slice(n * width, (n + 1) * width)
        p = dot(mix[...], weight_ref[:, at])
        wide[:, at] = p
        square = square + jnp.sum(p * p, axis=1, keepdims=True)
    scale = lax.rsqrt(square / out_ref.shape[1] + EPS)
    for n in range(out_ref.shape[1] // width):
        at = slice(n * width, (n + 1) * width)
        out_ref[:, at] = (wide[:, at] * scale * gain_ref[:, at]).astype(bf16)


def attention(first, sinks, queries, keys, values, rim, weight, gain):
    tokens, wide = queries.shape[0], weight.shape[1]
    lanes = 2 * HEAD_DIM
    rows = tokens + WINDOW
    return pl.pallas_call(
        attention_kernel,
        in_specs=[pl.BlockSpec(memory_space=pltpu.SMEM)] * 2 + in_vmem(6),
        out_specs=pl.BlockSpec(memory_space=VMEM),
        out_shape=jax.ShapeDtypeStruct((tokens, wide), bf16),
        scratch_shapes=[
            VMEM((KV_HEADS, rows, lanes), bf16),
            VMEM((KV_HEADS, rows, lanes), bf16),
            VMEM((tokens, HEADS * HEAD_DIM), bf16),
            VMEM((tokens, wide), f32),
        ],
        cost_estimate=pl.CostEstimate(
            flops=2 * tokens * HEADS * HEAD_DIM * (wide + 8 * WINDOW),
            bytes_accessed=2 * weight.size + 4 * tokens * wide,
            transcendentals=tokens * HEADS * 2 * WINDOW,
        ),
        compiler_params=pltpu.CompilerParams(vmem_limit_bytes=24 * MIB),
        name="attention",
    )(first, sinks, queries, keys, values, rim, weight, gain)


def body(
    att_queries,
    att_keys,
    att_values,
    sink_logits,
    out_weight,
    att_gain,
    moe_in,
    pre_gain,
    expert_ids,
    routed_expert_weight,
    w_gate,
    w_up,
    w_down,
    common_expert_gate_weight,
    common_expert_up_weight,
    common_expert_down_weight,
    moe_gain,
):
    x, core = lax.axis_index("tp"), lax.axis_index("c")
    tp = lax.axis_size("tp")
    near, far = [], []
    for i in range(tp):
        c = i // 2
        near += [(c * tp + (i - 1) % tp, c * tp + i), (c * tp + (i + 1) % tp, (1 - c) * tp + i)]
        far += [(c * tp + (i + 2) % tp, c * tp + i), (c * tp + i, (1 - c) * tp + i)]
    swapped = [(i, (i + tp) % (2 * tp)) for i in range(2 * tp)]
    own = (core == x // 2).astype(jnp.int32).reshape(1)

    kv_rows = jnp.stack([att_keys, att_values])
    rim_rows = from_behind(kv_rows[:, att_keys.shape[0] - WINDOW :], EP_TP, 1)
    first = (lax.axis_index(EP_TP) == 0).astype(jnp.int32).reshape(1)

    gate_t, up_t = w_gate.transpose(0, 2, 1), w_up.transpose(0, 2, 1)

    parity = (x % 2).astype(jnp.int32).reshape(1)

    def moved(piece, route):
        return lax.ppermute(piece, CORE_TP, route)

    def gathered(came_near, came_far, other_near, other_far):
        return (other_far, came_near, came_far, other_near), (
            came_far,
            other_near,
            other_far,
            came_near,
        )

    even, odd = pick(parity, (gate_t, up_t), 63)
    near_in, far_in = moved(odd, near), moved(even, far)

    ids_t = expert_ids.T
    packed, normed = pack(moe_in, pre_gain.reshape(1, -1), ids_t, 128 * CAP)
    chips = packed.shape[0] // (2 * CAP)
    arrived = lax.all_to_all(
        packed.reshape(chips, 2 * CAP, -1), CHIPS, split_axis=0, concat_axis=0, tiled=True
    ).reshape(packed.shape)

    even_out, odd_out = pick(parity, (w_down,), 8)
    near_out, far_out = moved(odd_out, near), moved(even_out, far)
    up_pieces = gathered(near_in, far_in, moved(near_in, swapped), moved(far_in, swapped))
    down_pieces = gathered(near_out, far_out, moved(near_out, swapped), moved(far_out, swapped))

    mixer_out = attention(
        first,
        sink_logits,
        att_queries,
        att_keys,
        att_values,
        rim_rows,
        out_weight,
        att_gain.reshape(1, -1),
    )

    hidden = expert_up(own, arrived, *up_pieces)
    out = expert_down(own, hidden, *down_pieces)
    returned = lax.all_to_all(
        out.reshape(chips, 2 * CAP, -1), CHIPS, split_axis=0, concat_axis=0, tiled=True
    ).reshape(out.shape)

    y, ys = lax.axis_index("y"), lax.axis_size("y")
    part = jnp.stack([2 * c + v for c in (core, 1 - core) for v in (y % 2, 1 - y % 2)])
    part = part.astype(jnp.int32)
    prepared = shared_prep(
        part,
        common_expert_gate_weight,
        common_expert_up_weight,
        common_expert_down_weight,
    )
    blocks = [prepared]
    for k in range(1, tp):
        blocks.append(lax.ppermute(prepared, "tp", [(i, (i + k) % tp) for i in range(tp)]))
    quarters = [jnp.concatenate(blocks, axis=0)]
    beside = [
        (2 * i + c, 2 * ((i + 1 - 2 * ((i + c) % 2)) % ys) + c) for i in range(ys) for c in range(2)
    ]
    quarters.append(lax.ppermute(quarters[0], ("y", "c"), beside))
    quarters += [lax.ppermute(v, "c", [(0, 1), (1, 0)]) for v in quarters]
    shared_sum, columns = shared_expert(
        part, ids_t, routed_expert_weight.T, normed, quarters
    )
    experts_out = combine(returned, shared_sum, columns, moe_gain.reshape(1, -1))
    return (mixer_out, experts_out)


def solution(mesh):
    split = Mesh(mesh.devices.reshape(8, 4, 2, mesh.shape["tp"]), ("z", "y", "c", "tp"))
    placed = (
        P(EP_TP, None),
        P(EP_TP, None),
        P(EP_TP, None),
        P(),
        P(),
        P(),
        P(EP_TP, None),
        P(),
        P(EP_TP, None),
        P(EP_TP, None),
        P(EP, None, "tp"),
        P(EP, None, "tp"),
        P(EP, "tp", None),
        P(None, "tp"),
        P(None, "tp"),
        P("tp", None),
        P(),
    )
    return jax.shard_map(
        body,
        mesh=split,
        in_specs=placed,
        out_specs=(P(EP_TP, None), P(EP_TP, None)),
        check_vma=False,
    )
```

```python
import math

import jax
import jax.numpy as jnp
from jax import lax
from jax.experimental import pallas as pl
from jax.experimental.pallas import tpu as pltpu
from jax.sharding import Mesh
from jax.sharding import PartitionSpec as P


HEADS = 16
KV_HEADS = 4
HEAD_DIM = 64
WINDOW = 128
CAP = 4
BLOCK = 256
MIB = 1 << 20
PARTS = 4
COMBINE_LIMIT = 62
UP_LIMIT = 24
DOWN_LIMIT = 16
EP = ("z", "y", "c")
EP_TP = ("z", "y", "c", "tp")
CHIPS = ("z", "y", "tp")
CORE_TP = ("c", "tp")
EPS = 1e-06
NEGATIVE = -1e30


f32 = jnp.float32
bf16 = jnp.bfloat16
VMEM = pltpu.VMEM
ANY = pl.ANY


def iota(shape, dim):
    return lax.broadcasted_iota(jnp.int32, shape, dim)


def dot(a, b):
    return jnp.dot(a, b, preferred_element_type=f32)


def dot_t(a, b):
    return lax.dot_general(a, b, (((1,), (1,)), ((), ())), preferred_element_type=f32)


def in_vmem(count):
    return [pl.BlockSpec(memory_space=VMEM)] * count


def from_behind(block, axis, distance):
    devices = range(lax.axis_size(axis))
    route = [(i - distance, i) for i in devices if i - distance in devices]
    return lax.ppermute(block, axis, route)


def rms_scale(inputs, gain_vec):
    mean_sq = jnp.mean(inputs * inputs, axis=-1, keepdims=True)
    return inputs * lax.rsqrt(mean_sq + EPS) * gain_vec


def slot_rows(ids, lanes):
    tokens = ids.shape[1]
    shape = (tokens, tokens)
    eye = iota(shape, 0) == iota(shape, 1)
    across = [ids[k : k + 1, :] for k in range(2)]
    down = [jnp.sum(jnp.where(eye, a, 0.0), axis=1, keepdims=True) for a in across]
    if lanes:
        mine, theirs, axis, earlier = across, down, 0, iota(shape, 0) < iota(shape, 1)
    else:
        mine, theirs, axis, earlier = down, across, 1, iota(shape, 1) < iota(shape, 0)
    rows = []
    for k in range(2):
        place = sum(
            jnp.sum(jnp.where((mine[k] == other) & earlier, 1.0, 0.0), axis=axis, keepdims=True)
            for other in theirs
        )
        rows.append((mine[k] * (2 * CAP) + place).astype(jnp.int32))
    return rows


def pack_kernel(
    expert_ref, x_ref, gain_ref, ids_ref, gate_ref, up_ref, packed_ref, normed_ref, piece_ref, *scratch
):
    stacked, made, held, sems, block_sems = scratch
    half = x_ref.shape[1] // 2
    tokens = x_ref.shape[0]
    ins, outs = expert_copies(expert_ref[0], (gate_ref, up_ref), held, piece_ref, sems)
    for c in ins:
        c.start()
    x = x_ref[...].astype(f32)
    normed = rms_scale(x, gain_ref[...]).astype(bf16)
    normed_ref[...] = normed
    stacked[:tokens, :] = normed[:, :half]
    stacked[tokens:, :] = normed[:, half:]
    rows = slot_rows(ids_ref[...].astype(f32), True)
    size = made.shape[0] // block_sems.shape[0]
    blocks = []
    for i in range(block_sems.shape[0]):
        at = pl.ds(i * size, size)
        blocks.append(pltpu.make_async_copy(made.at[at], packed_ref.at[at], block_sems.at[i]))
    for i, block in enumerate(blocks):
        r = iota((size, tokens), 0) + i * size
        chosen = jnp.concatenate(
            [
                jnp.where((r == rows[0] + h * CAP) | (r == rows[1] + h * CAP), 1.0, 0.0).astype(
                    bf16
                )
                for h in range(2)
            ],
            axis=1,
        )
        made[i * size : (i + 1) * size, :] = dot(chosen, stacked[...]).astype(bf16)
        block.start()
        if i == 0:
            for c, d in zip(ins, outs):
                c.wait()
                d.start()
    for c in blocks + outs:
        c.wait()


def pack(expert, x, gain, ids, gate, up, slots):
    tokens, width = x.shape
    rows = gate.shape[1]
    steps = 4
    total = 2 * slots
    hbm = pl.BlockSpec(memory_space=ANY)
    vmem = pl.BlockSpec(memory_space=VMEM)
    return pl.pallas_call(
        pack_kernel,
        in_specs=[pl.BlockSpec(memory_space=pltpu.SMEM), vmem, vmem, vmem, hbm, hbm],
        out_specs=[hbm, vmem, hbm],
        out_shape=[
            jax.ShapeDtypeStruct((total, width // 2), bf16),
            jax.ShapeDtypeStruct((tokens, width), bf16),
            jax.ShapeDtypeStruct((2 * rows, width), bf16),
        ],
        scratch_shapes=[
            VMEM((2 * tokens, width // 2), bf16),
            VMEM((total, width // 2), bf16),
            VMEM((2 * rows, width), bf16),
            pltpu.SemaphoreType.DMA((2, 2)),
            pltpu.SemaphoreType.DMA((steps,)),
        ],
        compiler_params=pltpu.CompilerParams(vmem_limit_bytes=63 * MIB),
        cost_estimate=pl.CostEstimate(
            flops=2 * total * tokens * width, bytes_accessed=6 * tokens * width, transcendentals=0
        ),
        name="pack",
    )(expert, x, gain, ids, gate, up)


def expert_copies(j, arrays, held, out, sems):
    rows = arrays[0].shape[1]
    ins, outs = [], []
    for m, array in enumerate(arrays):
        at = pl.ds(m * rows, rows)
        ins.append(pltpu.make_async_copy(array.at[j], held.at[at], sems.at[0, m]))
        outs.append(pltpu.make_async_copy(held.at[at], out.at[at], sems.at[1, m]))
    return ins, outs


def pick_kernel(expert_ref, *refs):
    ins, outs = expert_copies(expert_ref[0], refs[:-3], refs[-2], refs[-3], refs[-1])
    for c in ins:
        c.start()
    for c, d in zip(ins, outs):
        c.wait()
        d.start()
    for d in outs:
        d.wait()


def pick(expert, arrays, limit):
    rows, width = arrays[0].shape[1:]
    count = len(arrays)
    return pl.pallas_call(
        pick_kernel,
        in_specs=[pl.BlockSpec(memory_space=pltpu.SMEM)] + [pl.BlockSpec(memory_space=ANY)] * count,
        out_specs=pl.BlockSpec(memory_space=ANY),
        out_shape=jax.ShapeDtypeStruct((count * rows, width), bf16),
        scratch_shapes=[VMEM((count * rows, width), bf16), pltpu.SemaphoreType.DMA((2, count))],
        compiler_params=pltpu.CompilerParams(vmem_limit_bytes=limit * MIB),
        cost_estimate=pl.CostEstimate(
            flops=1000, bytes_accessed=4 * count * rows * width, transcendentals=0
        ),
        name="pick",
    )(expert, *arrays)


def start_pieces(own_ref, own, other, copy, parts):
    for mine, pieces in ((1, own), (0, other)):

        @pl.when(own_ref[0] == mine)
        def _():
            for m in range(parts):
                for k, piece in enumerate(pieces):
                    copy(k, m, piece).start()


def up_kernel(own_ref, recv, *refs):
    own, other = refs[:4], refs[4:8]
    hidden_ref, arrived, gate, up, rows, sem, sems = refs[8:]
    part = own[0].shape[0] // 2
    half = recv.shape[1]

    def copy(k, m, piece):
        return pltpu.make_async_copy(
            piece.at[pl.ds(m * part, part)], (gate, up)[m].at[pl.ds(k * part, part)], sems.at[m, k]
        )

    rows_in = pltpu.make_async_copy(recv, arrived, sem)
    rows_in.start()
    start_pieces(own_ref, own, other, copy, 2)
    a, b = iota((BLOCK // 2, BLOCK), 0), iota((BLOCK // 2, BLOCK), 1)
    first = (a // CAP) * (2 * CAP) + a % CAP
    picks = [jnp.where(b == first + h * CAP, 1.0, 0.0).astype(bf16) for h in range(2)]
    rows_in.wait()

    def sort_rows(i, carry):
        block = arrived[pl.ds(pl.multiple_of(i * BLOCK, BLOCK), BLOCK), :]
        at = pl.ds(pl.multiple_of(i * (BLOCK // 2), BLOCK // 2), BLOCK // 2)
        for h in range(2):
            rows[at, h * half : (h + 1) * half] = dot(picks[h], block).astype(bf16)
        return carry

    lax.fori_loop(0, recv.shape[0] // BLOCK, sort_rows, 0)
    for m in range(2):
        for k in range(4):
            copy(k, m, own[k]).wait()

    def units(n, carry):
        at = pl.ds(pl.multiple_of(n * BLOCK, BLOCK), BLOCK)
        x = rows[...]
        g = dot_t(x, gate[at, :])
        u = dot_t(x, up[at, :])
        hidden_ref[:, at] = (g / (1.0 + jnp.exp(-g)) * u).astype(bf16)
        return carry

    lax.fori_loop(0, hidden_ref.shape[1] // BLOCK, units, 0)


def expert_up(own, recv, mine, others):
    total, half = recv.shape
    units = 2 * mine[0].shape[0]
    return pl.pallas_call(
        up_kernel,
        in_specs=[pl.BlockSpec(memory_space=pltpu.SMEM)] + [pl.BlockSpec(memory_space=ANY)] * 9,
        out_specs=pl.BlockSpec(memory_space=VMEM),
        out_shape=jax.ShapeDtypeStruct((total // 2, units), bf16),
        scratch_shapes=[
            VMEM((total, half), bf16),
            VMEM((units, 2 * half), bf16),
            VMEM((units, 2 * half), bf16),
            VMEM((total // 2, 2 * half), bf16),
            pltpu.SemaphoreType.DMA,
            pltpu.SemaphoreType.DMA((2, 4)),
        ],
        compiler_params=pltpu.CompilerParams(vmem_limit_bytes=UP_LIMIT * MIB),
        cost_estimate=pl.CostEstimate(
            flops=4 * total * half * units,
            bytes_accessed=2 * total * half + 8 * half * units,
            transcendentals=total * units // 2,
        ),
        name="expert_up",
    )(own, recv, *mine, *others)


def down_kernel(own_ref, hidden, *refs):
    own, other = refs[:4], refs[4:8]
    out_ref, down, made, sems, out_sems = refs[8:]
    part = own[0].shape[0]
    half = out_ref.shape[1]
    count = half // BLOCK

    def copies(n, pieces):
        return [
            pltpu.make_async_copy(
                piece.at[:, pl.ds(h * half + n * BLOCK, BLOCK)],
                down.at[pl.ds(k * part, part), pl.ds(h * half + n * BLOCK, BLOCK)],
                sems.at[n, h, k],
            )
            for h in range(2)
            for k, piece in enumerate(pieces)
        ]

    for mine, pieces in ((1, own), (0, other)):

        @pl.when(own_ref[0] == mine)
        def _():
            for n in range(count):
                for c in copies(n, pieces):
                    c.start()

    tiles = hidden.shape[0] // (2 * CAP)
    low = iota((tiles, 2 * CAP, BLOCK), 1) < CAP
    for n in range(count):
        for c in copies(n, own):
            c.wait()
        at = n * BLOCK
        x = hidden[...]
        left = dot(x, down[:, at : at + BLOCK]).reshape(tiles, 2 * CAP, BLOCK)
        right = dot(x, down[:, half + at : half + at + BLOCK]).reshape(tiles, 2 * CAP, BLOCK)
        one = jnp.where(low, left, pltpu.roll(right, CAP, 1))
        two = jnp.where(low, pltpu.roll(left, CAP, 1), right)
        both = jnp.stack([one, two], axis=1).reshape(out_ref.shape[0], BLOCK)
        made[:, at : at + BLOCK] = both.astype(bf16)
        columns = pl.ds(at, BLOCK)
        pltpu.make_async_copy(made.at[:, columns], out_ref.at[:, columns], out_sems.at[n]).start()
    for n in range(count):
        columns = pl.ds(n * BLOCK, BLOCK)
        pltpu.make_async_copy(made.at[:, columns], out_ref.at[:, columns], out_sems.at[n]).wait()


def expert_down(own, hidden, mine, others):
    rows, units = hidden.shape
    width = mine[0].shape[1]
    count = width // 2 // BLOCK
    return pl.pallas_call(
        down_kernel,
        in_specs=[pl.BlockSpec(memory_space=pltpu.SMEM)]
        + in_vmem(1)
        + [pl.BlockSpec(memory_space=ANY)] * 8,
        out_specs=pl.BlockSpec(memory_space=ANY),
        out_shape=jax.ShapeDtypeStruct((2 * rows, width // 2), bf16),
        scratch_shapes=[
            VMEM((units, width), bf16),
            VMEM((2 * rows, width // 2), bf16),
            pltpu.SemaphoreType.DMA((count, 2, 4)),
            pltpu.SemaphoreType.DMA((count,)),
        ],
        compiler_params=pltpu.CompilerParams(vmem_limit_bytes=DOWN_LIMIT * MIB),
        cost_estimate=pl.CostEstimate(
            flops=2 * rows * units * width,
            bytes_accessed=2 * (rows * (units + width) + units * width),
            transcendentals=0,
        ),
        name="expert_down",
    )(own, hidden, *mine, *others)


def shared_prep_kernel(part_ref, gate_ref, up_ref, down_ref, out_ref):
    depth = gate_ref.shape[0] // PARTS
    units = gate_ref.shape[1]
    first = pl.multiple_of(part_ref[0] * depth, depth)
    at = pl.ds(first, depth)
    out_ref[:depth, :] = gate_ref[at, :]
    out_ref[depth : 2 * depth, :] = up_ref[at, :]
    for t in range(depth // 128):
        lane = pl.multiple_of(first + t * 128, 128)
        out_ref[2 * depth + t * units : 2 * depth + (t + 1) * units, :] = down_ref[
            :, pl.ds(lane, 128)
        ]


def shared_prep(part, gate, up, down):
    return pl.pallas_call(
        shared_prep_kernel,
        in_specs=[pl.BlockSpec(memory_space=pltpu.SMEM)] + in_vmem(3),
        out_specs=pl.BlockSpec(memory_space=VMEM),
        out_shape=jax.ShapeDtypeStruct((gate.shape[0] // PARTS * 3, gate.shape[1]), bf16),
        compiler_params=pltpu.CompilerParams(vmem_limit_bytes=8 * MIB),
        cost_estimate=pl.CostEstimate(flops=1000, bytes_accessed=8 * gate.size, transcendentals=0),
        name="shared_prep",
    )(part, gate, up, down)


def slot_columns(ids, weights):
    tokens = ids.shape[1]
    first = slot_rows(ids.astype(f32), False)
    eye = iota((tokens, tokens), 0) == iota((tokens, tokens), 1)
    lane = iota((tokens, 128), 1)
    out = jnp.zeros((tokens, 128), f32)
    for k in range(2):
        weight = jnp.sum(jnp.where(eye, weights[k : k + 1, :], 0.0), axis=1, keepdims=True)
        out = jnp.where(lane == k, first[k].astype(f32), out)
        out = jnp.where(lane == 2 + k, weight, out)
    return out


def shared_kernel(part_ref, ids_ref, weight_ref, x_ref, *refs):
    parts, (out_ref, columns_ref, into, down) = refs[:PARTS], refs[PARTS:]
    depth = x_ref.shape[1] // PARTS
    units = parts[0].shape[1]
    for p, ref in enumerate(parts):
        first = pl.multiple_of(part_ref[p] * depth, depth)
        for k in range(4):
            base = 3 * k * depth
            for m in range(2):
                lane = (m * 4 + k) * units
                into[pl.ds(first, depth), lane : lane + units] = ref[
                    base + m * depth : base + (m + 1) * depth, :
                ]
            for t in range(depth // 128):
                lane = pl.multiple_of(first + t * 128, 128)
                at = base + 2 * depth + t * units
                down[k * units : (k + 1) * units, pl.ds(lane, 128)] = ref[at : at + units, :]
    both = dot(x_ref[...], into[...])
    g, u = both[:, : 4 * units], both[:, 4 * units :]
    hidden = (g / (1.0 + jnp.exp(-g)) * u).astype(bf16)
    out_ref[...] = dot(hidden, down[...])
    columns_ref[...] = slot_columns(ids_ref[...], weight_ref[...])


def shared_expert(part, ids, weights, normed, parts):
    tokens, width = normed.shape
    units = 4 * parts[0].shape[1]
    return pl.pallas_call(
        shared_kernel,
        in_specs=[pl.BlockSpec(memory_space=pltpu.SMEM)] + in_vmem(3 + PARTS),
        out_specs=[pl.BlockSpec(memory_space=VMEM)] * 2,
        out_shape=[
            jax.ShapeDtypeStruct((tokens, width), f32),
            jax.ShapeDtypeStruct((tokens, 128), f32),
        ],
        scratch_shapes=[VMEM((width, 2 * units), bf16), VMEM((units, width), bf16)],
        compiler_params=pltpu.CompilerParams(vmem_limit_bytes=24 * MIB),
        cost_estimate=pl.CostEstimate(
            flops=6 * tokens * width * units,
            bytes_accessed=6 * width * units,
            transcendentals=tokens * units,
        ),
        name="shared_expert",
    )(part, ids, weights, normed, *parts)


def combine_kernel(
    back_ref, shared_ref, columns_ref, gain_ref, out_ref, came, common, sem, back_sems
):
    tokens, half = out_ref.shape[0], back_ref.shape[1]
    rows = [pl.ds(i * BLOCK, BLOCK) for i in range(back_ref.shape[0] // BLOCK)]
    back_in = [
        pltpu.make_async_copy(back_ref.at[at], came.at[at], back_sems.at[i])
        for i, at in enumerate(rows)
    ]
    shared_in = pltpu.make_async_copy(shared_ref, common, sem)
    for c in back_in:
        c.start()
    shared_in.start()
    r = iota((tokens, back_ref.shape[0]), 1)
    first = [columns_ref[:, k : k + 1].astype(jnp.int32) for k in range(2)]
    weights = [columns_ref[:, 2 + k : 3 + k] for k in range(2)]
    spreads = []
    for h in range(2):
        spread = jnp.where(r == first[0] + h * CAP, weights[0], 0.0) + jnp.where(
            r == first[1] + h * CAP, weights[1], 0.0
        )
        spreads.append(spread.astype(bf16))
    spread = jnp.concatenate(spreads, axis=0)
    summed = jnp.zeros((2 * tokens, half), f32)
    for i, c in enumerate(back_in):
        c.wait()
        at = slice(i * BLOCK, (i + 1) * BLOCK)
        summed = summed + dot(spread[:, at], came[at, :])
    shared_in.wait()
    halves = [
        summed[h * tokens : (h + 1) * tokens] + common[:, h * half : (h + 1) * half]
        for h in range(2)
    ]
    square = sum(jnp.sum(v * v, axis=1, keepdims=True) for v in halves)
    scale = lax.rsqrt(square / (2 * half) + EPS)
    for h, v in enumerate(halves):
        at = slice(h * half, (h + 1) * half)
        out_ref[:, at] = (v * scale * gain_ref[:, at]).astype(bf16)


def combine(back, shared, columns, gain):
    slots, half = back.shape
    tokens = shared.shape[0]
    return pl.pallas_call(
        combine_kernel,
        in_specs=[pl.BlockSpec(memory_space=ANY)] * 2 + in_vmem(2),
        out_specs=pl.BlockSpec(memory_space=VMEM),
        out_shape=jax.ShapeDtypeStruct((tokens, 2 * half), bf16),
        scratch_shapes=[
            VMEM((slots, half), bf16),
            VMEM((tokens, 2 * half), f32),
            pltpu.SemaphoreType.DMA,
            pltpu.SemaphoreType.DMA((slots // BLOCK,)),
        ],
        compiler_params=pltpu.CompilerParams(vmem_limit_bytes=COMBINE_LIMIT * MIB),
        cost_estimate=pl.CostEstimate(
            flops=8 * tokens * slots * half, bytes_accessed=2 * slots * half, transcendentals=0
        ),
        name="combine",
    )(back, shared, columns, gain)


def attention_kernel(
    first_ref, sink_ref, q_ref, k_ref, v_ref, rim_ref, weight_ref, gain_ref, out_ref, keys, values, mix, wide
):
    tokens = q_ref.shape[0]
    lanes = 2 * HEAD_DIM
    group = HEADS // KV_HEADS
    tiles = k_ref.shape[1] // lanes
    for into, rim, own in ((keys, 0, k_ref), (values, 1, v_ref)):
        for t in range(tiles):
            at = slice(t * lanes, (t + 1) * lanes)
            rows = jnp.concatenate([rim_ref[rim, :, at], own[:, at]], axis=0)
            into[2 * t] = rows
            into[2 * t + 1] = jnp.concatenate([rows[:, HEAD_DIM:], rows[:, :HEAD_DIM]], axis=1)
    i, j = iota((WINDOW, 2 * WINDOW), 0), iota((WINDOW, 2 * WINDOW), 1)
    low = iota((WINDOW, lanes), 1) < HEAD_DIM

    for n in range(tokens // WINDOW):
        band = slice(n * WINDOW, (n + 2) * WINDOW)
        at = slice(n * WINDOW, (n + 1) * WINDOW)
        inside = (j > i) & (j <= i + WINDOW)
        if n == 0:
            inside = inside & (j >= first_ref[0] * WINDOW)
        for g in range(KV_HEADS):
            kt = [2 * (g // 2) + (g + s) % 2 for s in range(2)]
            for t in range(group // 2):
                tile = g * (group // 2) + t
                q = q_ref[at, tile * lanes : (tile + 1) * lanes]
                mixed = []
                for s in range(2):
                    mine = jnp.where(low if s == 0 else ~low, q, jnp.zeros_like(q))
                    score = dot_t(mine, keys[kt[s], band, :]) * (1.0 / math.sqrt(HEAD_DIM))
                    score = jnp.where(inside, score, NEGATIVE)
                    sink = sink_ref[2 * tile + s]
                    top = jnp.maximum(jnp.max(score, axis=1, keepdims=True), sink)
                    e = jnp.exp(score - top)
                    below = jnp.sum(e, axis=1, keepdims=True) + jnp.exp(sink - top)
                    mixed.append(dot((e / below).astype(bf16), values[kt[s], band, :]))
                mix[at, tile * lanes : (tile + 1) * lanes] = jnp.where(
                    low, mixed[0], mixed[1]
                ).astype(bf16)

    width = 512
    square = jnp.zeros((tokens, 1), f32)
    for n in range(out_ref.shape[1] // width):
        at = slice(n * width, (n + 1) * width)
        p = dot(mix[...], weight_ref[:, at])
        wide[:, at] = p
        square = square + jnp.sum(p * p, axis=1, keepdims=True)
    scale = lax.rsqrt(square / out_ref.shape[1] + EPS)
    for n in range(out_ref.shape[1] // width):
        at = slice(n * width, (n + 1) * width)
        out_ref[:, at] = (wide[:, at] * scale * gain_ref[:, at]).astype(bf16)


def attention(first, sinks, queries, keys, values, rim, weight, gain):
    tokens, wide = queries.shape[0], weight.shape[1]
    lanes = 2 * HEAD_DIM
    rows = tokens + WINDOW
    return pl.pallas_call(
        attention_kernel,
        in_specs=[pl.BlockSpec(memory_space=pltpu.SMEM)] * 2 + in_vmem(6),
        out_specs=pl.BlockSpec(memory_space=VMEM),
        out_shape=jax.ShapeDtypeStruct((tokens, wide), bf16),
        scratch_shapes=[
            VMEM((KV_HEADS, rows, lanes), bf16),
            VMEM((KV_HEADS, rows, lanes), bf16),
            VMEM((tokens, HEADS * HEAD_DIM), bf16),
            VMEM((tokens, wide), f32),
        ],
        cost_estimate=pl.CostEstimate(
            flops=2 * tokens * HEADS * HEAD_DIM * (wide + 8 * WINDOW),
            bytes_accessed=2 * weight.size + 4 * tokens * wide,
            transcendentals=tokens * HEADS * 2 * WINDOW,
        ),
        compiler_params=pltpu.CompilerParams(vmem_limit_bytes=24 * MIB),
        name="attention",
    )(first, sinks, queries, keys, values, rim, weight, gain)


def body(
    att_queries,
    att_keys,
    att_values,
    sink_logits,
    out_weight,
    att_gain,
    moe_in,
    pre_gain,
    expert_ids,
    routed_expert_weight,
    w_gate,
    w_up,
    w_down,
    common_expert_gate_weight,
    common_expert_up_weight,
    common_expert_down_weight,
    moe_gain,
):
    x, core = lax.axis_index("tp"), lax.axis_index("c")
    tp = lax.axis_size("tp")
    near, far = [], []
    for i in range(tp):
        c = i // 2
        near += [(c * tp + (i - 1) % tp, c * tp + i), (c * tp + (i + 1) % tp, (1 - c) * tp + i)]
        far += [(c * tp + (i + 2) % tp, c * tp + i), (c * tp + i, (1 - c) * tp + i)]
    swapped = [(i, (i + tp) % (2 * tp)) for i in range(2 * tp)]
    own = (core == x // 2).astype(jnp.int32).reshape(1)

    kv_rows = jnp.stack([att_keys, att_values])
    rim_rows = from_behind(kv_rows[:, att_keys.shape[0] - WINDOW :], EP_TP, 1)
    first = (lax.axis_index(EP_TP) == 0).astype(jnp.int32).reshape(1)

    gate_t, up_t = w_gate.transpose(0, 2, 1), w_up.transpose(0, 2, 1)

    even_expert = (x % 2).astype(jnp.int32).reshape(1)
    odd_expert = 1 - even_expert

    def moved(piece, route):
        return lax.ppermute(piece, CORE_TP, route)

    def gathered(came_near, came_far, other_near, other_far):
        return (other_far, came_near, came_far, other_near), (
            came_far,
            other_near,
            other_far,
            came_near,
        )

    near_in = moved(pick(odd_expert, (gate_t, up_t), 63), near)
    ids_t = expert_ids.T
    packed, normed, even = pack(
        even_expert, moe_in, pre_gain.reshape(1, -1), ids_t, gate_t, up_t, 128 * CAP
    )
    far_in = moved(even, far)
    chips = packed.shape[0] // (2 * CAP)
    arrived = lax.all_to_all(
        packed.reshape(chips, 2 * CAP, -1), CHIPS, split_axis=0, concat_axis=0, tiled=True
    ).reshape(packed.shape)

    near_out = moved(pick(odd_expert, (w_down,), 8), near)
    far_out = moved(pick(even_expert, (w_down,), 8), far)
    up_pieces = gathered(near_in, far_in, moved(near_in, swapped), moved(far_in, swapped))
    down_pieces = gathered(near_out, far_out, moved(near_out, swapped), moved(far_out, swapped))

    mixer_out = attention(
        first,
        sink_logits,
        att_queries,
        att_keys,
        att_values,
        rim_rows,
        out_weight,
        att_gain.reshape(1, -1),
    )

    hidden = expert_up(own, arrived, *up_pieces)
    out = expert_down(own, hidden, *down_pieces)
    returned = lax.all_to_all(
        out.reshape(chips, 2 * CAP, -1), CHIPS, split_axis=0, concat_axis=0, tiled=True
    ).reshape(out.shape)

    y, ys = lax.axis_index("y"), lax.axis_size("y")
    part = jnp.stack([2 * c + v for c in (core, 1 - core) for v in (y % 2, 1 - y % 2)])
    part = part.astype(jnp.int32)
    prepared = shared_prep(
        part,
        common_expert_gate_weight,
        common_expert_up_weight,
        common_expert_down_weight,
    )
    blocks = [prepared]
    for k in range(1, tp):
        blocks.append(lax.ppermute(prepared, "tp", [(i, (i + k) % tp) for i in range(tp)]))
    quarters = [jnp.concatenate(blocks, axis=0)]
    beside = [
        (2 * i + c, 2 * ((i + 1 - 2 * ((i + c) % 2)) % ys) + c) for i in range(ys) for c in range(2)
    ]
    quarters.append(lax.ppermute(quarters[0], ("y", "c"), beside))
    quarters += [lax.ppermute(v, "c", [(0, 1), (1, 0)]) for v in quarters]
    shared_sum, columns = shared_expert(
        part, ids_t, routed_expert_weight.T, normed, quarters
    )
    experts_out = combine(returned, shared_sum, columns, moe_gain.reshape(1, -1))
    return (mixer_out, experts_out)


def solution(mesh):
    split = Mesh(mesh.devices.reshape(8, 4, 2, mesh.shape["tp"]), ("z", "y", "c", "tp"))
    placed = (
        P(EP_TP, None),
        P(EP_TP, None),
        P(EP_TP, None),
        P(),
        P(),
        P(),
        P(EP_TP, None),
        P(),
        P(EP_TP, None),
        P(EP_TP, None),
        P(EP, None, "tp"),
        P(EP, None, "tp"),
        P(EP, "tp", None),
        P(None, "tp"),
        P(None, "tp"),
        P("tp", None),
        P(),
    )
    return jax.shard_map(
        body,
        mesh=split,
        in_specs=placed,
        out_specs=(P(EP_TP, None), P(EP_TP, None)),
        check_vma=False,
    )
```

```python
import math

import jax
import jax.numpy as jnp
from jax import lax
from jax.experimental import pallas as pl
from jax.experimental.pallas import tpu as pltpu
from jax.sharding import Mesh
from jax.sharding import PartitionSpec as P


HEADS = 16
KV_HEADS = 4
HEAD_DIM = 64
WINDOW = 128
CAP = 4
BLOCK = 256
MIB = 1 << 20
PARTS = 4
COMBINE_LIMIT = 16
UP_LIMIT = 24
DOWN_LIMIT = 16
EP = ("z", "y", "c")
EP_TP = ("z", "y", "c", "tp")
CHIPS = ("z", "y", "tp")
CORE_TP = ("c", "tp")
EPS = 1e-06
NEGATIVE = -1e30


f32 = jnp.float32
bf16 = jnp.bfloat16
VMEM = pltpu.VMEM
ANY = pl.ANY


def iota(shape, dim):
    return lax.broadcasted_iota(jnp.int32, shape, dim)


def dot(a, b):
    return jnp.dot(a, b, preferred_element_type=f32)


def dot_t(a, b):
    return lax.dot_general(a, b, (((1,), (1,)), ((), ())), preferred_element_type=f32)


def in_vmem(count):
    return [pl.BlockSpec(memory_space=VMEM)] * count


def from_behind(block, axis, distance):
    devices = range(lax.axis_size(axis))
    route = [(i - distance, i) for i in devices if i - distance in devices]
    return lax.ppermute(block, axis, route)


def rms_scale(inputs, gain_vec):
    mean_sq = jnp.mean(inputs * inputs, axis=-1, keepdims=True)
    return inputs * lax.rsqrt(mean_sq + EPS) * gain_vec


def slot_rows(ids, lanes):
    tokens = ids.shape[1]
    shape = (tokens, tokens)
    eye = iota(shape, 0) == iota(shape, 1)
    across = [ids[k : k + 1, :] for k in range(2)]
    down = [jnp.sum(jnp.where(eye, a, 0.0), axis=1, keepdims=True) for a in across]
    if lanes:
        mine, theirs, axis, earlier = across, down, 0, iota(shape, 0) < iota(shape, 1)
    else:
        mine, theirs, axis, earlier = down, across, 1, iota(shape, 1) < iota(shape, 0)
    rows = []
    for k in range(2):
        place = sum(
            jnp.sum(jnp.where((mine[k] == other) & earlier, 1.0, 0.0), axis=axis, keepdims=True)
            for other in theirs
        )
        rows.append((mine[k] * (2 * CAP) + place).astype(jnp.int32))
    return rows


def pack_kernel(
    expert_ref, x_ref, gain_ref, ids_ref, gate_ref, up_ref, packed_ref, normed_ref, piece_ref, *scratch
):
    stacked, made, held, sems, block_sems = scratch
    half = x_ref.shape[1] // 2
    tokens = x_ref.shape[0]
    ins, outs = expert_copies(expert_ref[0], (gate_ref, up_ref), held, piece_ref, sems)
    for c in ins:
        c.start()
    x = x_ref[...].astype(f32)
    normed = rms_scale(x, gain_ref[...]).astype(bf16)
    normed_ref[...] = normed
    stacked[:tokens, :] = normed[:, :half]
    stacked[tokens:, :] = normed[:, half:]
    rows = slot_rows(ids_ref[...].astype(f32), True)
    size = made.shape[0] // block_sems.shape[0]
    blocks = []
    for i in range(block_sems.shape[0]):
        at = pl.ds(i * size, size)
        blocks.append(pltpu.make_async_copy(made.at[at], packed_ref.at[at], block_sems.at[i]))
    for i, block in enumerate(blocks):
        r = iota((size, tokens), 0) + i * size
        chosen = jnp.concatenate(
            [
                jnp.where((r == rows[0] + h * CAP) | (r == rows[1] + h * CAP), 1.0, 0.0).astype(
                    bf16
                )
                for h in range(2)
            ],
            axis=1,
        )
        made[i * size : (i + 1) * size, :] = dot(chosen, stacked[...]).astype(bf16)
        block.start()
        if i == 0:
            for c, d in zip(ins, outs):
                c.wait()
                d.start()
    for c in blocks + outs:
        c.wait()


def pack(expert, x, gain, ids, gate, up, slots):
    tokens, width = x.shape
    rows = gate.shape[1]
    steps = 4
    total = 2 * slots
    hbm = pl.BlockSpec(memory_space=ANY)
    vmem = pl.BlockSpec(memory_space=VMEM)
    return pl.pallas_call(
        pack_kernel,
        in_specs=[pl.BlockSpec(memory_space=pltpu.SMEM), vmem, vmem, vmem, hbm, hbm],
        out_specs=[hbm, vmem, hbm],
        out_shape=[
            jax.ShapeDtypeStruct((total, width // 2), bf16),
            jax.ShapeDtypeStruct((tokens, width), bf16),
            jax.ShapeDtypeStruct((2 * rows, width), bf16),
        ],
        scratch_shapes=[
            VMEM((2 * tokens, width // 2), bf16),
            VMEM((total, width // 2), bf16),
            VMEM((2 * rows, width), bf16),
            pltpu.SemaphoreType.DMA((2, 2)),
            pltpu.SemaphoreType.DMA((steps,)),
        ],
        compiler_params=pltpu.CompilerParams(vmem_limit_bytes=63 * MIB),
        cost_estimate=pl.CostEstimate(
            flops=2 * total * tokens * width, bytes_accessed=6 * tokens * width, transcendentals=0
        ),
        name="pack",
    )(expert, x, gain, ids, gate, up)


def expert_copies(j, arrays, held, out, sems):
    rows = arrays[0].shape[1]
    ins, outs = [], []
    for m, array in enumerate(arrays):
        at = pl.ds(m * rows, rows)
        ins.append(pltpu.make_async_copy(array.at[j], held.at[at], sems.at[0, m]))
        outs.append(pltpu.make_async_copy(held.at[at], out.at[at], sems.at[1, m]))
    return ins, outs


def pick_kernel(expert_ref, *refs):
    ins, outs = expert_copies(expert_ref[0], refs[:-3], refs[-2], refs[-3], refs[-1])
    for c in ins:
        c.start()
    for c, d in zip(ins, outs):
        c.wait()
        d.start()
    for d in outs:
        d.wait()


def pick(expert, arrays, limit):
    rows, width = arrays[0].shape[1:]
    count = len(arrays)
    return pl.pallas_call(
        pick_kernel,
        in_specs=[pl.BlockSpec(memory_space=pltpu.SMEM)] + [pl.BlockSpec(memory_space=ANY)] * count,
        out_specs=pl.BlockSpec(memory_space=ANY),
        out_shape=jax.ShapeDtypeStruct((count * rows, width), bf16),
        scratch_shapes=[VMEM((count * rows, width), bf16), pltpu.SemaphoreType.DMA((2, count))],
        compiler_params=pltpu.CompilerParams(vmem_limit_bytes=limit * MIB),
        cost_estimate=pl.CostEstimate(
            flops=1000, bytes_accessed=4 * count * rows * width, transcendentals=0
        ),
        name="pick",
    )(expert, *arrays)


def start_pieces(own_ref, own, other, copy, parts):
    for mine, pieces in ((1, own), (0, other)):

        @pl.when(own_ref[0] == mine)
        def _():
            for m in range(parts):
                for k, piece in enumerate(pieces):
                    copy(k, m, piece).start()


def up_kernel(own_ref, recv, *refs):
    own, other = refs[:4], refs[4:8]
    hidden_ref, arrived, gate, up, rows, sem, sems = refs[8:]
    part = own[0].shape[0] // 2
    half = recv.shape[1]

    def copy(k, m, piece):
        return pltpu.make_async_copy(
            piece.at[pl.ds(m * part, part)], (gate, up)[m].at[pl.ds(k * part, part)], sems.at[m, k]
        )

    rows_in = pltpu.make_async_copy(recv, arrived, sem)
    rows_in.start()
    start_pieces(own_ref, own, other, copy, 2)
    a, b = iota((BLOCK // 2, BLOCK), 0), iota((BLOCK // 2, BLOCK), 1)
    first = (a // CAP) * (2 * CAP) + a % CAP
    picks = [jnp.where(b == first + h * CAP, 1.0, 0.0).astype(bf16) for h in range(2)]
    rows_in.wait()

    def sort_rows(i, carry):
        block = arrived[pl.ds(pl.multiple_of(i * BLOCK, BLOCK), BLOCK), :]
        at = pl.ds(pl.multiple_of(i * (BLOCK // 2), BLOCK // 2), BLOCK // 2)
        for h in range(2):
            rows[at, h * half : (h + 1) * half] = dot(picks[h], block).astype(bf16)
        return carry

    lax.fori_loop(0, recv.shape[0] // BLOCK, sort_rows, 0)
    for m in range(2):
        for k in range(4):
            copy(k, m, own[k]).wait()

    def units(n, carry):
        at = pl.ds(pl.multiple_of(n * BLOCK, BLOCK), BLOCK)
        x = rows[...]
        g = dot_t(x, gate[at, :])
        u = dot_t(x, up[at, :])
        hidden_ref[:, at] = (g / (1.0 + jnp.exp(-g)) * u).astype(bf16)
        return carry

    lax.fori_loop(0, hidden_ref.shape[1] // BLOCK, units, 0)


def expert_up(own, recv, mine, others):
    total, half = recv.shape
    units = 2 * mine[0].shape[0]
    return pl.pallas_call(
        up_kernel,
        in_specs=[pl.BlockSpec(memory_space=pltpu.SMEM)] + [pl.BlockSpec(memory_space=ANY)] * 9,
        out_specs=pl.BlockSpec(memory_space=VMEM),
        out_shape=jax.ShapeDtypeStruct((total // 2, units), bf16),
        scratch_shapes=[
            VMEM((total, half), bf16),
            VMEM((units, 2 * half), bf16),
            VMEM((units, 2 * half), bf16),
            VMEM((total // 2, 2 * half), bf16),
            pltpu.SemaphoreType.DMA,
            pltpu.SemaphoreType.DMA((2, 4)),
        ],
        compiler_params=pltpu.CompilerParams(vmem_limit_bytes=UP_LIMIT * MIB),
        cost_estimate=pl.CostEstimate(
            flops=4 * total * half * units,
            bytes_accessed=2 * total * half + 8 * half * units,
            transcendentals=total * units // 2,
        ),
        name="expert_up",
    )(own, recv, *mine, *others)


def down_kernel(own_ref, hidden, *refs):
    own, other = refs[:4], refs[4:8]
    out_ref, down, made, sems, out_sems = refs[8:]
    part = own[0].shape[0]
    half = out_ref.shape[1]
    count = half // BLOCK

    def copies(n, pieces):
        return [
            pltpu.make_async_copy(
                piece.at[:, pl.ds(h * half + n * BLOCK, BLOCK)],
                down.at[pl.ds(k * part, part), pl.ds(h * half + n * BLOCK, BLOCK)],
                sems.at[n, h, k],
            )
            for h in range(2)
            for k, piece in enumerate(pieces)
        ]

    for mine, pieces in ((1, own), (0, other)):

        @pl.when(own_ref[0] == mine)
        def _():
            for n in range(count):
                for c in copies(n, pieces):
                    c.start()

    tiles = hidden.shape[0] // (2 * CAP)
    low = iota((tiles, 2 * CAP, BLOCK), 1) < CAP
    for n in range(count):
        for c in copies(n, own):
            c.wait()
        at = n * BLOCK
        x = hidden[...]
        left = dot(x, down[:, at : at + BLOCK]).reshape(tiles, 2 * CAP, BLOCK)
        right = dot(x, down[:, half + at : half + at + BLOCK]).reshape(tiles, 2 * CAP, BLOCK)
        one = jnp.where(low, left, pltpu.roll(right, CAP, 1))
        two = jnp.where(low, pltpu.roll(left, CAP, 1), right)
        both = jnp.stack([one, two], axis=1).reshape(out_ref.shape[0], BLOCK)
        made[:, at : at + BLOCK] = both.astype(bf16)
        columns = pl.ds(at, BLOCK)
        pltpu.make_async_copy(made.at[:, columns], out_ref.at[:, columns], out_sems.at[n]).start()
    for n in range(count):
        columns = pl.ds(n * BLOCK, BLOCK)
        pltpu.make_async_copy(made.at[:, columns], out_ref.at[:, columns], out_sems.at[n]).wait()


def expert_down(own, hidden, mine, others):
    rows, units = hidden.shape
    width = mine[0].shape[1]
    count = width // 2 // BLOCK
    return pl.pallas_call(
        down_kernel,
        in_specs=[pl.BlockSpec(memory_space=pltpu.SMEM)]
        + in_vmem(1)
        + [pl.BlockSpec(memory_space=ANY)] * 8,
        out_specs=pl.BlockSpec(memory_space=ANY),
        out_shape=jax.ShapeDtypeStruct((2 * rows, width // 2), bf16),
        scratch_shapes=[
            VMEM((units, width), bf16),
            VMEM((2 * rows, width // 2), bf16),
            pltpu.SemaphoreType.DMA((count, 2, 4)),
            pltpu.SemaphoreType.DMA((count,)),
        ],
        compiler_params=pltpu.CompilerParams(vmem_limit_bytes=DOWN_LIMIT * MIB),
        cost_estimate=pl.CostEstimate(
            flops=2 * rows * units * width,
            bytes_accessed=2 * (rows * (units + width) + units * width),
            transcendentals=0,
        ),
        name="expert_down",
    )(own, hidden, *mine, *others)


def shared_prep_kernel(part_ref, gate_ref, up_ref, down_ref, out_ref):
    depth = gate_ref.shape[0] // PARTS
    units = gate_ref.shape[1]
    first = pl.multiple_of(part_ref[0] * depth, depth)
    at = pl.ds(first, depth)
    out_ref[:depth, :] = gate_ref[at, :]
    out_ref[depth : 2 * depth, :] = up_ref[at, :]
    for t in range(depth // 128):
        lane = pl.multiple_of(first + t * 128, 128)
        out_ref[2 * depth + t * units : 2 * depth + (t + 1) * units, :] = down_ref[
            :, pl.ds(lane, 128)
        ]


def shared_prep(part, gate, up, down):
    return pl.pallas_call(
        shared_prep_kernel,
        in_specs=[pl.BlockSpec(memory_space=pltpu.SMEM)] + in_vmem(3),
        out_specs=pl.BlockSpec(memory_space=VMEM),
        out_shape=jax.ShapeDtypeStruct((gate.shape[0] // PARTS * 3, gate.shape[1]), bf16),
        compiler_params=pltpu.CompilerParams(vmem_limit_bytes=8 * MIB),
        cost_estimate=pl.CostEstimate(flops=1000, bytes_accessed=8 * gate.size, transcendentals=0),
        name="shared_prep",
    )(part, gate, up, down)


def slot_columns(ids, weights):
    tokens = ids.shape[1]
    first = slot_rows(ids.astype(f32), False)
    eye = iota((tokens, tokens), 0) == iota((tokens, tokens), 1)
    lane = iota((tokens, 128), 1)
    out = jnp.zeros((tokens, 128), f32)
    for k in range(2):
        weight = jnp.sum(jnp.where(eye, weights[k : k + 1, :], 0.0), axis=1, keepdims=True)
        out = jnp.where(lane == k, first[k].astype(f32), out)
        out = jnp.where(lane == 2 + k, weight, out)
    return out


def shared_kernel(part_ref, ids_ref, weight_ref, x_ref, *refs):
    most, last = refs[:PARTS], refs[PARTS : 2 * PARTS]
    out_ref, columns_ref, into, down = refs[2 * PARTS :]
    depth = x_ref.shape[1] // PARTS
    units = most[0].shape[1]
    for p in range(PARTS):
        first = pl.multiple_of(part_ref[p] * depth, depth)
        for k in range(4):
            ref, base = (most[p], 3 * k * depth) if k < 3 else (last[p], 0)
            for m in range(2):
                lane = (m * 4 + k) * units
                into[pl.ds(first, depth), lane : lane + units] = ref[
                    base + m * depth : base + (m + 1) * depth, :
                ]
            for t in range(depth // 128):
                lane = pl.multiple_of(first + t * 128, 128)
                at = base + 2 * depth + t * units
                down[k * units : (k + 1) * units, pl.ds(lane, 128)] = ref[at : at + units, :]
    both = dot(x_ref[...], into[...])
    g, u = both[:, : 4 * units], both[:, 4 * units :]
    hidden = (g / (1.0 + jnp.exp(-g)) * u).astype(bf16)
    out_ref[...] = dot(hidden, down[...])
    columns_ref[...] = slot_columns(ids_ref[...], weight_ref[...])


def shared_expert(part, ids, weights, normed, most, last):
    tokens, width = normed.shape
    units = 4 * most[0].shape[1]
    return pl.pallas_call(
        shared_kernel,
        in_specs=[pl.BlockSpec(memory_space=pltpu.SMEM)] + in_vmem(3 + 2 * PARTS),
        out_specs=[pl.BlockSpec(memory_space=VMEM)] * 2,
        out_shape=[
            jax.ShapeDtypeStruct((tokens, width), f32),
            jax.ShapeDtypeStruct((tokens, 128), f32),
        ],
        scratch_shapes=[VMEM((width, 2 * units), bf16), VMEM((units, width), bf16)],
        compiler_params=pltpu.CompilerParams(vmem_limit_bytes=24 * MIB),
        cost_estimate=pl.CostEstimate(
            flops=6 * tokens * width * units,
            bytes_accessed=6 * width * units,
            transcendentals=tokens * units,
        ),
        name="shared_expert",
    )(part, ids, weights, normed, *most, *last)


def combine_kernel(back_ref, shared_ref, columns_ref, gain_ref, out_ref):
    tokens, half = out_ref.shape[0], back_ref.shape[1]
    r = iota((tokens, back_ref.shape[0]), 1)
    first = [columns_ref[:, k : k + 1].astype(jnp.int32) for k in range(2)]
    weights = [columns_ref[:, 2 + k : 3 + k] for k in range(2)]
    spreads = []
    for h in range(2):
        spread = jnp.where(r == first[0] + h * CAP, weights[0], 0.0) + jnp.where(
            r == first[1] + h * CAP, weights[1], 0.0
        )
        spreads.append(spread.astype(bf16))
    spread = jnp.concatenate(spreads, axis=0)
    summed = dot(spread, back_ref[...])
    halves = [
        summed[h * tokens : (h + 1) * tokens] + shared_ref[:, h * half : (h + 1) * half]
        for h in range(2)
    ]
    square = sum(jnp.sum(v * v, axis=1, keepdims=True) for v in halves)
    scale = lax.rsqrt(square / (2 * half) + EPS)
    for h, v in enumerate(halves):
        at = slice(h * half, (h + 1) * half)
        out_ref[:, at] = (v * scale * gain_ref[:, at]).astype(bf16)


def combine(back, shared, columns, gain):
    slots, half = back.shape
    tokens = shared.shape[0]
    return pl.pallas_call(
        combine_kernel,
        in_specs=in_vmem(4),
        out_specs=pl.BlockSpec(memory_space=VMEM),
        out_shape=jax.ShapeDtypeStruct((tokens, 2 * half), bf16),
        compiler_params=pltpu.CompilerParams(vmem_limit_bytes=COMBINE_LIMIT * MIB),
        cost_estimate=pl.CostEstimate(
            flops=8 * tokens * slots * half, bytes_accessed=2 * slots * half, transcendentals=0
        ),
        name="combine",
    )(back, shared, columns, gain)


def attention_kernel(
    first_ref, sink_ref, q_ref, k_ref, v_ref, rim_ref, weight_ref, gain_ref, out_ref, keys, values, mix, wide
):
    tokens = q_ref.shape[0]
    lanes = 2 * HEAD_DIM
    group = HEADS // KV_HEADS
    tiles = k_ref.shape[1] // lanes
    for into, rim, own in ((keys, 0, k_ref), (values, 1, v_ref)):
        for t in range(tiles):
            at = slice(t * lanes, (t + 1) * lanes)
            rows = jnp.concatenate([rim_ref[rim, :, at], own[:, at]], axis=0)
            into[2 * t] = rows
            into[2 * t + 1] = jnp.concatenate([rows[:, HEAD_DIM:], rows[:, :HEAD_DIM]], axis=1)
    i, j = iota((WINDOW, 2 * WINDOW), 0), iota((WINDOW, 2 * WINDOW), 1)
    low = iota((WINDOW, lanes), 1) < HEAD_DIM

    for n in range(tokens // WINDOW):
        band = slice(n * WINDOW, (n + 2) * WINDOW)
        at = slice(n * WINDOW, (n + 1) * WINDOW)
        inside = (j > i) & (j <= i + WINDOW)
        if n == 0:
            inside = inside & (j >= first_ref[0] * WINDOW)
        for g in range(KV_HEADS):
            kt = [2 * (g // 2) + (g + s) % 2 for s in range(2)]
            for t in range(group // 2):
                tile = g * (group // 2) + t
                q = q_ref[at, tile * lanes : (tile + 1) * lanes]
                mixed = []
                for s in range(2):
                    mine = jnp.where(low if s == 0 else ~low, q, jnp.zeros_like(q))
                    score = dot_t(mine, keys[kt[s], band, :]) * (1.0 / math.sqrt(HEAD_DIM))
                    score = jnp.where(inside, score, NEGATIVE)
                    sink = sink_ref[2 * tile + s]
                    top = jnp.maximum(jnp.max(score, axis=1, keepdims=True), sink)
                    e = jnp.exp(score - top)
                    below = jnp.sum(e, axis=1, keepdims=True) + jnp.exp(sink - top)
                    mixed.append(dot((e / below).astype(bf16), values[kt[s], band, :]))
                mix[at, tile * lanes : (tile + 1) * lanes] = jnp.where(
                    low, mixed[0], mixed[1]
                ).astype(bf16)

    width = 512
    square = jnp.zeros((tokens, 1), f32)
    for n in range(out_ref.shape[1] // width):
        at = slice(n * width, (n + 1) * width)
        p = dot(mix[...], weight_ref[:, at])
        wide[:, at] = p
        square = square + jnp.sum(p * p, axis=1, keepdims=True)
    scale = lax.rsqrt(square / out_ref.shape[1] + EPS)
    for n in range(out_ref.shape[1] // width):
        at = slice(n * width, (n + 1) * width)
        out_ref[:, at] = (wide[:, at] * scale * gain_ref[:, at]).astype(bf16)


def attention(first, sinks, queries, keys, values, rim, weight, gain):
    tokens, wide = queries.shape[0], weight.shape[1]
    lanes = 2 * HEAD_DIM
    rows = tokens + WINDOW
    return pl.pallas_call(
        attention_kernel,
        in_specs=[pl.BlockSpec(memory_space=pltpu.SMEM)] * 2 + in_vmem(6),
        out_specs=pl.BlockSpec(memory_space=VMEM),
        out_shape=jax.ShapeDtypeStruct((tokens, wide), bf16),
        scratch_shapes=[
            VMEM((KV_HEADS, rows, lanes), bf16),
            VMEM((KV_HEADS, rows, lanes), bf16),
            VMEM((tokens, HEADS * HEAD_DIM), bf16),
            VMEM((tokens, wide), f32),
        ],
        cost_estimate=pl.CostEstimate(
            flops=2 * tokens * HEADS * HEAD_DIM * (wide + 8 * WINDOW),
            bytes_accessed=2 * weight.size + 4 * tokens * wide,
            transcendentals=tokens * HEADS * 2 * WINDOW,
        ),
        compiler_params=pltpu.CompilerParams(vmem_limit_bytes=24 * MIB),
        name="attention",
    )(first, sinks, queries, keys, values, rim, weight, gain)


def body(
    att_queries,
    att_keys,
    att_values,
    sink_logits,
    out_weight,
    att_gain,
    moe_in,
    pre_gain,
    expert_ids,
    routed_expert_weight,
    w_gate,
    w_up,
    w_down,
    common_expert_gate_weight,
    common_expert_up_weight,
    common_expert_down_weight,
    moe_gain,
):
    x, core = lax.axis_index("tp"), lax.axis_index("c")
    tp = lax.axis_size("tp")
    near, far = [], []
    for i in range(tp):
        c = i // 2
        near += [(c * tp + (i - 1) % tp, c * tp + i), (c * tp + (i + 1) % tp, (1 - c) * tp + i)]
        far += [(c * tp + (i + 2) % tp, c * tp + i), (c * tp + i, (1 - c) * tp + i)]
    swapped = [(i, (i + tp) % (2 * tp)) for i in range(2 * tp)]
    own = (core == x // 2).astype(jnp.int32).reshape(1)

    kv_rows = jnp.stack([att_keys, att_values])
    rim_rows = from_behind(kv_rows[:, att_keys.shape[0] - WINDOW :], EP_TP, 1)
    first = (lax.axis_index(EP_TP) == 0).astype(jnp.int32).reshape(1)

    gate_t, up_t = w_gate.transpose(0, 2, 1), w_up.transpose(0, 2, 1)

    even_expert = (x % 2).astype(jnp.int32).reshape(1)
    odd_expert = 1 - even_expert

    def moved(piece, route):
        return lax.ppermute(piece, CORE_TP, route)

    def gathered(came_near, came_far, other_near, other_far):
        return (other_far, came_near, came_far, other_near), (
            came_far,
            other_near,
            other_far,
            came_near,
        )

    near_in = moved(pick(odd_expert, (gate_t, up_t), 63), near)
    ids_t = expert_ids.T
    packed, normed, even = pack(
        even_expert, moe_in, pre_gain.reshape(1, -1), ids_t, gate_t, up_t, 128 * CAP
    )
    far_in = moved(even, far)
    chips = packed.shape[0] // (2 * CAP)
    arrived = lax.all_to_all(
        packed.reshape(chips, 2 * CAP, -1), CHIPS, split_axis=0, concat_axis=0, tiled=True
    ).reshape(packed.shape)

    near_out = moved(pick(odd_expert, (w_down,), 8), near)
    far_out = moved(pick(even_expert, (w_down,), 8), far)
    up_pieces = gathered(near_in, far_in, moved(near_in, swapped), moved(far_in, swapped))
    down_pieces = gathered(near_out, far_out, moved(near_out, swapped), moved(far_out, swapped))

    mixer_out = attention(
        first,
        sink_logits,
        att_queries,
        att_keys,
        att_values,
        rim_rows,
        out_weight,
        att_gain.reshape(1, -1),
    )

    hidden = expert_up(own, arrived, *up_pieces)
    out = expert_down(own, hidden, *down_pieces)
    returned = lax.all_to_all(
        out.reshape(chips, 2 * CAP, -1), CHIPS, split_axis=0, concat_axis=0, tiled=True
    ).reshape(out.shape)

    y, ys = lax.axis_index("y"), lax.axis_size("y")
    part = jnp.stack([2 * c + v for c in (core, 1 - core) for v in (y % 2, 1 - y % 2)])
    part = part.astype(jnp.int32)
    prepared = shared_prep(
        part,
        common_expert_gate_weight,
        common_expert_up_weight,
        common_expert_down_weight,
    )
    crossed = {}
    for k in (1, 3, 2):
        crossed[k] = lax.ppermute(prepared, "tp", [(i, (i + k) % tp) for i in range(tp)])
    beside = [
        (2 * i + c, 2 * ((i + 1 - 2 * ((i + c) % 2)) % ys) + c) for i in range(ys) for c in range(2)
    ]

    def spread_out(piece):
        pair = [piece, lax.ppermute(piece, ("y", "c"), beside)]
        return pair + [lax.ppermute(v, "c", [(0, 1), (1, 0)]) for v in pair]

    most = spread_out(jnp.concatenate([prepared, crossed[1], crossed[3]], axis=0))
    rest = spread_out(crossed[2])
    shared_sum, columns = shared_expert(
        part, ids_t, routed_expert_weight.T, normed, most, rest
    )
    experts_out = combine(returned, shared_sum, columns, moe_gain.reshape(1, -1))
    return (mixer_out, experts_out)


def solution(mesh):
    split = Mesh(mesh.devices.reshape(8, 4, 2, mesh.shape["tp"]), ("z", "y", "c", "tp"))
    placed = (
        P(EP_TP, None),
        P(EP_TP, None),
        P(EP_TP, None),
        P(),
        P(),
        P(),
        P(EP_TP, None),
        P(),
        P(EP_TP, None),
        P(EP_TP, None),
        P(EP, None, "tp"),
        P(EP, None, "tp"),
        P(EP, "tp", None),
        P(None, "tp"),
        P(None, "tp"),
        P("tp", None),
        P(),
    )
    return jax.shard_map(
        body,
        mesh=split,
        in_specs=placed,
        out_specs=(P(EP_TP, None), P(EP_TP, None)),
        check_vma=False,
    )
```

```python
import math

import jax
import jax.numpy as jnp
from jax import lax
from jax.experimental import pallas as pl
from jax.experimental.pallas import tpu as pltpu
from jax.sharding import Mesh
from jax.sharding import PartitionSpec as P


HEADS = 16
KV_HEADS = 4
HEAD_DIM = 64
WINDOW = 128
CAP = 4
BLOCK = 256
MIB = 1 << 20
PARTS = 4
COMBINE_LIMIT = 16
UP_LIMIT = 24
DOWN_LIMIT = 16
EP = ("z", "y", "c")
EP_TP = ("z", "y", "c", "tp")
CHIPS = ("tp", "z", "y")
CORE_TP = ("c", "tp")
EPS = 1e-06
NEGATIVE = -1e30


f32 = jnp.float32
bf16 = jnp.bfloat16
VMEM = pltpu.VMEM
ANY = pl.ANY


def iota(shape, dim):
    return lax.broadcasted_iota(jnp.int32, shape, dim)


def dot(a, b):
    return jnp.dot(a, b, preferred_element_type=f32)


def dot_t(a, b):
    return lax.dot_general(a, b, (((1,), (1,)), ((), ())), preferred_element_type=f32)


def in_vmem(count):
    return [pl.BlockSpec(memory_space=VMEM)] * count


def from_behind(block, axis, distance):
    devices = range(lax.axis_size(axis))
    route = [(i - distance, i) for i in devices if i - distance in devices]
    return lax.ppermute(block, axis, route)


def rms_scale(inputs, gain_vec):
    mean_sq = jnp.mean(inputs * inputs, axis=-1, keepdims=True)
    return inputs * lax.rsqrt(mean_sq + EPS) * gain_vec


def chip_index(ids):
    return (ids & 3) * 32 + (ids >> 4) * 4 + ((ids >> 2) & 3)


def slot_rows(ids, lanes):
    tokens = ids.shape[1]
    shape = (tokens, tokens)
    eye = iota(shape, 0) == iota(shape, 1)
    across = [ids[k : k + 1, :] for k in range(2)]
    down = [jnp.sum(jnp.where(eye, a, 0.0), axis=1, keepdims=True) for a in across]
    if lanes:
        mine, theirs, axis, earlier = across, down, 0, iota(shape, 0) < iota(shape, 1)
    else:
        mine, theirs, axis, earlier = down, across, 1, iota(shape, 1) < iota(shape, 0)
    rows = []
    for k in range(2):
        place = sum(
            jnp.sum(jnp.where((mine[k] == other) & earlier, 1.0, 0.0), axis=axis, keepdims=True)
            for other in theirs
        )
        rows.append((mine[k] * (2 * CAP) + place).astype(jnp.int32))
    return rows


def pack_kernel(
    expert_ref, x_ref, gain_ref, ids_ref, gate_ref, up_ref, packed_ref, normed_ref, piece_ref, *scratch
):
    stacked, made, held, sems, block_sems = scratch
    half = x_ref.shape[1] // 2
    tokens = x_ref.shape[0]
    ins, outs = expert_copies(expert_ref[0], (gate_ref, up_ref), held, piece_ref, sems)
    for c in ins:
        c.start()
    x = x_ref[...].astype(f32)
    normed = rms_scale(x, gain_ref[...]).astype(bf16)
    normed_ref[...] = normed
    stacked[:tokens, :] = normed[:, :half]
    stacked[tokens:, :] = normed[:, half:]
    rows = slot_rows(chip_index(ids_ref[...]).astype(f32), True)
    size = made.shape[0] // block_sems.shape[0]
    blocks = []
    for i in range(block_sems.shape[0]):
        at = pl.ds(i * size, size)
        blocks.append(pltpu.make_async_copy(made.at[at], packed_ref.at[at], block_sems.at[i]))
    for i, block in enumerate(blocks):
        r = iota((size, tokens), 0) + i * size
        chosen = jnp.concatenate(
            [
                jnp.where((r == rows[0] + h * CAP) | (r == rows[1] + h * CAP), 1.0, 0.0).astype(
                    bf16
                )
                for h in range(2)
            ],
            axis=1,
        )
        made[i * size : (i + 1) * size, :] = dot(chosen, stacked[...]).astype(bf16)
        block.start()
        if i == 0:
            for c, d in zip(ins, outs):
                c.wait()
                d.start()
    for c in blocks + outs:
        c.wait()


def pack(expert, x, gain, ids, gate, up, slots):
    tokens, width = x.shape
    rows = gate.shape[1]
    steps = 4
    total = 2 * slots
    hbm = pl.BlockSpec(memory_space=ANY)
    vmem = pl.BlockSpec(memory_space=VMEM)
    return pl.pallas_call(
        pack_kernel,
        in_specs=[pl.BlockSpec(memory_space=pltpu.SMEM), vmem, vmem, vmem, hbm, hbm],
        out_specs=[hbm, vmem, hbm],
        out_shape=[
            jax.ShapeDtypeStruct((total, width // 2), bf16),
            jax.ShapeDtypeStruct((tokens, width), bf16),
            jax.ShapeDtypeStruct((2 * rows, width), bf16),
        ],
        scratch_shapes=[
            VMEM((2 * tokens, width // 2), bf16),
            VMEM((total, width // 2), bf16),
            VMEM((2 * rows, width), bf16),
            pltpu.SemaphoreType.DMA((2, 2)),
            pltpu.SemaphoreType.DMA((steps,)),
        ],
        compiler_params=pltpu.CompilerParams(vmem_limit_bytes=63 * MIB),
        cost_estimate=pl.CostEstimate(
            flops=2 * total * tokens * width, bytes_accessed=6 * tokens * width, transcendentals=0
        ),
        name="pack",
    )(expert, x, gain, ids, gate, up)


def expert_copies(j, arrays, held, out, sems):
    rows = arrays[0].shape[1]
    ins, outs = [], []
    for m, array in enumerate(arrays):
        at = pl.ds(m * rows, rows)
        ins.append(pltpu.make_async_copy(array.at[j], held.at[at], sems.at[0, m]))
        outs.append(pltpu.make_async_copy(held.at[at], out.at[at], sems.at[1, m]))
    return ins, outs


def pick_kernel(expert_ref, *refs):
    ins, outs = expert_copies(expert_ref[0], refs[:-3], refs[-2], refs[-3], refs[-1])
    for c in ins:
        c.start()
    for c, d in zip(ins, outs):
        c.wait()
        d.start()
    for d in outs:
        d.wait()


def pick(expert, arrays, limit):
    rows, width = arrays[0].shape[1:]
    count = len(arrays)
    return pl.pallas_call(
        pick_kernel,
        in_specs=[pl.BlockSpec(memory_space=pltpu.SMEM)] + [pl.BlockSpec(memory_space=ANY)] * count,
        out_specs=pl.BlockSpec(memory_space=ANY),
        out_shape=jax.ShapeDtypeStruct((count * rows, width), bf16),
        scratch_shapes=[VMEM((count * rows, width), bf16), pltpu.SemaphoreType.DMA((2, count))],
        compiler_params=pltpu.CompilerParams(vmem_limit_bytes=limit * MIB),
        cost_estimate=pl.CostEstimate(
            flops=1000, bytes_accessed=4 * count * rows * width, transcendentals=0
        ),
        name="pick",
    )(expert, *arrays)


def start_pieces(own_ref, own, other, copy, parts):
    for mine, pieces in ((1, own), (0, other)):

        @pl.when(own_ref[0] == mine)
        def _():
            for m in range(parts):
                for k, piece in enumerate(pieces):
                    copy(k, m, piece).start()


def up_kernel(own_ref, recv, *refs):
    own, other = refs[:4], refs[4:8]
    hidden_ref, arrived, gate, up, rows, sem, sems = refs[8:]
    part = own[0].shape[0] // 2
    half = recv.shape[1]

    def copy(k, m, piece):
        return pltpu.make_async_copy(
            piece.at[pl.ds(m * part, part)], (gate, up)[m].at[pl.ds(k * part, part)], sems.at[m, k]
        )

    rows_in = pltpu.make_async_copy(recv, arrived, sem)
    rows_in.start()
    start_pieces(own_ref, own, other, copy, 2)
    a, b = iota((BLOCK // 2, BLOCK), 0), iota((BLOCK // 2, BLOCK), 1)
    first = (a // CAP) * (2 * CAP) + a % CAP
    picks = [jnp.where(b == first + h * CAP, 1.0, 0.0).astype(bf16) for h in range(2)]
    rows_in.wait()

    def sort_rows(i, carry):
        block = arrived[pl.ds(pl.multiple_of(i * BLOCK, BLOCK), BLOCK), :]
        at = pl.ds(pl.multiple_of(i * (BLOCK // 2), BLOCK // 2), BLOCK // 2)
        for h in range(2):
            rows[at, h * half : (h + 1) * half] = dot(picks[h], block).astype(bf16)
        return carry

    lax.fori_loop(0, recv.shape[0] // BLOCK, sort_rows, 0)
    for m in range(2):
        for k in range(4):
            copy(k, m, own[k]).wait()

    def units(n, carry):
        at = pl.ds(pl.multiple_of(n * BLOCK, BLOCK), BLOCK)
        x = rows[...]
        g = dot_t(x, gate[at, :])
        u = dot_t(x, up[at, :])
        hidden_ref[:, at] = (g / (1.0 + jnp.exp(-g)) * u).astype(bf16)
        return carry

    lax.fori_loop(0, hidden_ref.shape[1] // BLOCK, units, 0)


def expert_up(own, recv, mine, others):
    total, half = recv.shape
    units = 2 * mine[0].shape[0]
    return pl.pallas_call(
        up_kernel,
        in_specs=[pl.BlockSpec(memory_space=pltpu.SMEM)] + [pl.BlockSpec(memory_space=ANY)] * 9,
        out_specs=pl.BlockSpec(memory_space=VMEM),
        out_shape=jax.ShapeDtypeStruct((total // 2, units), bf16),
        scratch_shapes=[
            VMEM((total, half), bf16),
            VMEM((units, 2 * half), bf16),
            VMEM((units, 2 * half), bf16),
            VMEM((total // 2, 2 * half), bf16),
            pltpu.SemaphoreType.DMA,
            pltpu.SemaphoreType.DMA((2, 4)),
        ],
        compiler_params=pltpu.CompilerParams(vmem_limit_bytes=UP_LIMIT * MIB),
        cost_estimate=pl.CostEstimate(
            flops=4 * total * half * units,
            bytes_accessed=2 * total * half + 8 * half * units,
            transcendentals=total * units // 2,
        ),
        name="expert_up",
    )(own, recv, *mine, *others)


def down_kernel(own_ref, hidden, *refs):
    own, other = refs[:4], refs[4:8]
    out_ref, down, made, sems, out_sems = refs[8:]
    part = own[0].shape[0]
    half = out_ref.shape[1]
    count = half // BLOCK

    def copies(n, pieces):
        return [
            pltpu.make_async_copy(
                piece.at[:, pl.ds(h * half + n * BLOCK, BLOCK)],
                down.at[pl.ds(k * part, part), pl.ds(h * half + n * BLOCK, BLOCK)],
                sems.at[n, h, k],
            )
            for h in range(2)
            for k, piece in enumerate(pieces)
        ]

    for mine, pieces in ((1, own), (0, other)):

        @pl.when(own_ref[0] == mine)
        def _():
            for n in range(count):
                for c in copies(n, pieces):
                    c.start()

    tiles = hidden.shape[0] // (2 * CAP)
    low = iota((tiles, 2 * CAP, BLOCK), 1) < CAP
    for n in range(count):
        for c in copies(n, own):
            c.wait()
        at = n * BLOCK
        x = hidden[...]
        left = dot(x, down[:, at : at + BLOCK]).reshape(tiles, 2 * CAP, BLOCK)
        right = dot(x, down[:, half + at : half + at + BLOCK]).reshape(tiles, 2 * CAP, BLOCK)
        one = jnp.where(low, left, pltpu.roll(right, CAP, 1))
        two = jnp.where(low, pltpu.roll(left, CAP, 1), right)
        both = jnp.stack([one, two], axis=1).reshape(out_ref.shape[0], BLOCK)
        made[:, at : at + BLOCK] = both.astype(bf16)
        columns = pl.ds(at, BLOCK)
        pltpu.make_async_copy(made.at[:, columns], out_ref.at[:, columns], out_sems.at[n]).start()
    for n in range(count):
        columns = pl.ds(n * BLOCK, BLOCK)
        pltpu.make_async_copy(made.at[:, columns], out_ref.at[:, columns], out_sems.at[n]).wait()


def expert_down(own, hidden, mine, others):
    rows, units = hidden.shape
    width = mine[0].shape[1]
    count = width // 2 // BLOCK
    return pl.pallas_call(
        down_kernel,
        in_specs=[pl.BlockSpec(memory_space=pltpu.SMEM)]
        + in_vmem(1)
        + [pl.BlockSpec(memory_space=ANY)] * 8,
        out_specs=pl.BlockSpec(memory_space=ANY),
        out_shape=jax.ShapeDtypeStruct((2 * rows, width // 2), bf16),
        scratch_shapes=[
            VMEM((units, width), bf16),
            VMEM((2 * rows, width // 2), bf16),
            pltpu.SemaphoreType.DMA((count, 2, 4)),
            pltpu.SemaphoreType.DMA((count,)),
        ],
        compiler_params=pltpu.CompilerParams(vmem_limit_bytes=DOWN_LIMIT * MIB),
        cost_estimate=pl.CostEstimate(
            flops=2 * rows * units * width,
            bytes_accessed=2 * (rows * (units + width) + units * width),
            transcendentals=0,
        ),
        name="expert_down",
    )(own, hidden, *mine, *others)


def shared_prep_kernel(part_ref, gate_ref, up_ref, down_ref, out_ref):
    depth = gate_ref.shape[0] // PARTS
    units = gate_ref.shape[1]
    first = pl.multiple_of(part_ref[0] * depth, depth)
    at = pl.ds(first, depth)
    out_ref[:depth, :] = gate_ref[at, :]
    out_ref[depth : 2 * depth, :] = up_ref[at, :]
    for t in range(depth // 128):
        lane = pl.multiple_of(first + t * 128, 128)
        out_ref[2 * depth + t * units : 2 * depth + (t + 1) * units, :] = down_ref[
            :, pl.ds(lane, 128)
        ]


def shared_prep(part, gate, up, down):
    return pl.pallas_call(
        shared_prep_kernel,
        in_specs=[pl.BlockSpec(memory_space=pltpu.SMEM)] + in_vmem(3),
        out_specs=pl.BlockSpec(memory_space=VMEM),
        out_shape=jax.ShapeDtypeStruct((gate.shape[0] // PARTS * 3, gate.shape[1]), bf16),
        compiler_params=pltpu.CompilerParams(vmem_limit_bytes=8 * MIB),
        cost_estimate=pl.CostEstimate(flops=1000, bytes_accessed=8 * gate.size, transcendentals=0),
        name="shared_prep",
    )(part, gate, up, down)


def slot_columns(ids, weights):
    tokens = ids.shape[1]
    first = slot_rows(chip_index(ids).astype(f32), False)
    eye = iota((tokens, tokens), 0) == iota((tokens, tokens), 1)
    lane = iota((tokens, 128), 1)
    out = jnp.zeros((tokens, 128), f32)
    for k in range(2):
        weight = jnp.sum(jnp.where(eye, weights[k : k + 1, :], 0.0), axis=1, keepdims=True)
        out = jnp.where(lane == k, first[k].astype(f32), out)
        out = jnp.where(lane == 2 + k, weight, out)
    return out


def shared_kernel(part_ref, ids_ref, weight_ref, x_ref, *refs):
    most, last = refs[:PARTS], refs[PARTS : 2 * PARTS]
    out_ref, columns_ref, into, down = refs[2 * PARTS :]
    depth = x_ref.shape[1] // PARTS
    units = most[0].shape[1]
    for p in range(PARTS):
        first = pl.multiple_of(part_ref[p] * depth, depth)
        for k in range(4):
            ref, base = (most[p], 3 * k * depth) if k < 3 else (last[p], 0)
            for m in range(2):
                lane = (m * 4 + k) * units
                into[pl.ds(first, depth), lane : lane + units] = ref[
                    base + m * depth : base + (m + 1) * depth, :
                ]
            for t in range(depth // 128):
                lane = pl.multiple_of(first + t * 128, 128)
                at = base + 2 * depth + t * units
                down[k * units : (k + 1) * units, pl.ds(lane, 128)] = ref[at : at + units, :]
    both = dot(x_ref[...], into[...])
    g, u = both[:, : 4 * units], both[:, 4 * units :]
    hidden = (g / (1.0 + jnp.exp(-g)) * u).astype(bf16)
    out_ref[...] = dot(hidden, down[...])
    columns_ref[...] = slot_columns(ids_ref[...], weight_ref[...])


def shared_expert(part, ids, weights, normed, most, last):
    tokens, width = normed.shape
    units = 4 * most[0].shape[1]
    return pl.pallas_call(
        shared_kernel,
        in_specs=[pl.BlockSpec(memory_space=pltpu.SMEM)] + in_vmem(3 + 2 * PARTS),
        out_specs=[pl.BlockSpec(memory_space=VMEM)] * 2,
        out_shape=[
            jax.ShapeDtypeStruct((tokens, width), f32),
            jax.ShapeDtypeStruct((tokens, 128), f32),
        ],
        scratch_shapes=[VMEM((width, 2 * units), bf16), VMEM((units, width), bf16)],
        compiler_params=pltpu.CompilerParams(vmem_limit_bytes=24 * MIB),
        cost_estimate=pl.CostEstimate(
            flops=6 * tokens * width * units,
            bytes_accessed=6 * width * units,
            transcendentals=tokens * units,
        ),
        name="shared_expert",
    )(part, ids, weights, normed, *most, *last)


def combine_kernel(back_ref, shared_ref, columns_ref, gain_ref, out_ref):
    tokens, half = out_ref.shape[0], back_ref.shape[1]
    r = iota((tokens, back_ref.shape[0]), 1)
    first = [columns_ref[:, k : k + 1].astype(jnp.int32) for k in range(2)]
    weights = [columns_ref[:, 2 + k : 3 + k] for k in range(2)]
    spreads = []
    for h in range(2):
        spread = jnp.where(r == first[0] + h * CAP, weights[0], 0.0) + jnp.where(
            r == first[1] + h * CAP, weights[1], 0.0
        )
        spreads.append(spread.astype(bf16))
    spread = jnp.concatenate(spreads, axis=0)
    summed = dot(spread, back_ref[...])
    halves = [
        summed[h * tokens : (h + 1) * tokens] + shared_ref[:, h * half : (h + 1) * half]
        for h in range(2)
    ]
    square = sum(jnp.sum(v * v, axis=1, keepdims=True) for v in halves)
    scale = lax.rsqrt(square / (2 * half) + EPS)
    for h, v in enumerate(halves):
        at = slice(h * half, (h + 1) * half)
        out_ref[:, at] = (v * scale * gain_ref[:, at]).astype(bf16)


def combine(back, shared, columns, gain):
    slots, half = back.shape
    tokens = shared.shape[0]
    return pl.pallas_call(
        combine_kernel,
        in_specs=in_vmem(4),
        out_specs=pl.BlockSpec(memory_space=VMEM),
        out_shape=jax.ShapeDtypeStruct((tokens, 2 * half), bf16),
        compiler_params=pltpu.CompilerParams(vmem_limit_bytes=COMBINE_LIMIT * MIB),
        cost_estimate=pl.CostEstimate(
            flops=8 * tokens * slots * half, bytes_accessed=2 * slots * half, transcendentals=0
        ),
        name="combine",
    )(back, shared, columns, gain)


def attention_kernel(
    first_ref, sink_ref, q_ref, k_ref, v_ref, rim_ref, weight_ref, gain_ref, out_ref, keys, values, mix, wide
):
    tokens = q_ref.shape[0]
    lanes = 2 * HEAD_DIM
    group = HEADS // KV_HEADS
    tiles = k_ref.shape[1] // lanes
    for into, rim, own in ((keys, 0, k_ref), (values, 1, v_ref)):
        for t in range(tiles):
            at = slice(t * lanes, (t + 1) * lanes)
            rows = jnp.concatenate([rim_ref[rim, :, at], own[:, at]], axis=0)
            into[2 * t] = rows
            into[2 * t + 1] = jnp.concatenate([rows[:, HEAD_DIM:], rows[:, :HEAD_DIM]], axis=1)
    i, j = iota((WINDOW, 2 * WINDOW), 0), iota((WINDOW, 2 * WINDOW), 1)
    low = iota((WINDOW, lanes), 1) < HEAD_DIM

    for n in range(tokens // WINDOW):
        band = slice(n * WINDOW, (n + 2) * WINDOW)
        at = slice(n * WINDOW, (n + 1) * WINDOW)
        inside = (j > i) & (j <= i + WINDOW)
        if n == 0:
            inside = inside & (j >= first_ref[0] * WINDOW)
        for g in range(KV_HEADS):
            kt = [2 * (g // 2) + (g + s) % 2 for s in range(2)]
            for t in range(group // 2):
                tile = g * (group // 2) + t
                q = q_ref[at, tile * lanes : (tile + 1) * lanes]
                mixed = []
                for s in range(2):
                    mine = jnp.where(low if s == 0 else ~low, q, jnp.zeros_like(q))
                    score = dot_t(mine, keys[kt[s], band, :]) * (1.0 / math.sqrt(HEAD_DIM))
                    score = jnp.where(inside, score, NEGATIVE)
                    sink = sink_ref[2 * tile + s]
                    top = jnp.maximum(jnp.max(score, axis=1, keepdims=True), sink)
                    e = jnp.exp(score - top)
                    below = jnp.sum(e, axis=1, keepdims=True) + jnp.exp(sink - top)
                    mixed.append(dot((e / below).astype(bf16), values[kt[s], band, :]))
                mix[at, tile * lanes : (tile + 1) * lanes] = jnp.where(
                    low, mixed[0], mixed[1]
                ).astype(bf16)

    width = 512
    square = jnp.zeros((tokens, 1), f32)
    for n in range(out_ref.shape[1] // width):
        at = slice(n * width, (n + 1) * width)
        p = dot(mix[...], weight_ref[:, at])
        wide[:, at] = p
        square = square + jnp.sum(p * p, axis=1, keepdims=True)
    scale = lax.rsqrt(square / out_ref.shape[1] + EPS)
    for n in range(out_ref.shape[1] // width):
        at = slice(n * width, (n + 1) * width)
        out_ref[:, at] = (wide[:, at] * scale * gain_ref[:, at]).astype(bf16)


def attention(first, sinks, queries, keys, values, rim, weight, gain):
    tokens, wide = queries.shape[0], weight.shape[1]
    lanes = 2 * HEAD_DIM
    rows = tokens + WINDOW
    return pl.pallas_call(
        attention_kernel,
        in_specs=[pl.BlockSpec(memory_space=pltpu.SMEM)] * 2 + in_vmem(6),
        out_specs=pl.BlockSpec(memory_space=VMEM),
        out_shape=jax.ShapeDtypeStruct((tokens, wide), bf16),
        scratch_shapes=[
            VMEM((KV_HEADS, rows, lanes), bf16),
            VMEM((KV_HEADS, rows, lanes), bf16),
            VMEM((tokens, HEADS * HEAD_DIM), bf16),
            VMEM((tokens, wide), f32),
        ],
        cost_estimate=pl.CostEstimate(
            flops=2 * tokens * HEADS * HEAD_DIM * (wide + 8 * WINDOW),
            bytes_accessed=2 * weight.size + 4 * tokens * wide,
            transcendentals=tokens * HEADS * 2 * WINDOW,
        ),
        compiler_params=pltpu.CompilerParams(vmem_limit_bytes=24 * MIB),
        name="attention",
    )(first, sinks, queries, keys, values, rim, weight, gain)


def body(
    att_queries,
    att_keys,
    att_values,
    sink_logits,
    out_weight,
    att_gain,
    moe_in,
    pre_gain,
    expert_ids,
    routed_expert_weight,
    w_gate,
    w_up,
    w_down,
    common_expert_gate_weight,
    common_expert_up_weight,
    common_expert_down_weight,
    moe_gain,
):
    x, core = lax.axis_index("tp"), lax.axis_index("c")
    tp = lax.axis_size("tp")
    near, far = [], []
    for i in range(tp):
        c = i // 2
        near += [(c * tp + (i - 1) % tp, c * tp + i), (c * tp + (i + 1) % tp, (1 - c) * tp + i)]
        far += [(c * tp + (i + 2) % tp, c * tp + i), (c * tp + i, (1 - c) * tp + i)]
    swapped = [(i, (i + tp) % (2 * tp)) for i in range(2 * tp)]
    own = (core == x // 2).astype(jnp.int32).reshape(1)

    kv_rows = jnp.stack([att_keys, att_values])
    rim_rows = from_behind(kv_rows[:, att_keys.shape[0] - WINDOW :], EP_TP, 1)
    first = (lax.axis_index(EP_TP) == 0).astype(jnp.int32).reshape(1)

    gate_t, up_t = w_gate.transpose(0, 2, 1), w_up.transpose(0, 2, 1)

    even_expert = (x % 2).astype(jnp.int32).reshape(1)
    odd_expert = 1 - even_expert

    def moved(piece, route):
        return lax.ppermute(piece, CORE_TP, route)

    def gathered(came_near, came_far, other_near, other_far):
        return (other_far, came_near, came_far, other_near), (
            came_far,
            other_near,
            other_far,
            came_near,
        )

    near_in = moved(pick(odd_expert, (gate_t, up_t), 63), near)
    ids_t = expert_ids.T
    packed, normed, even = pack(
        even_expert, moe_in, pre_gain.reshape(1, -1), ids_t, gate_t, up_t, 128 * CAP
    )
    far_in = moved(even, far)
    chips = packed.shape[0] // (2 * CAP)
    arrived = lax.all_to_all(
        packed.reshape(chips, 2 * CAP, -1), CHIPS, split_axis=0, concat_axis=0, tiled=True
    ).reshape(packed.shape)

    near_out = moved(pick(odd_expert, (w_down,), 8), near)
    far_out = moved(pick(even_expert, (w_down,), 8), far)
    up_pieces = gathered(near_in, far_in, moved(near_in, swapped), moved(far_in, swapped))
    down_pieces = gathered(near_out, far_out, moved(near_out, swapped), moved(far_out, swapped))

    mixer_out = attention(
        first,
        sink_logits,
        att_queries,
        att_keys,
        att_values,
        rim_rows,
        out_weight,
        att_gain.reshape(1, -1),
    )

    hidden = expert_up(own, arrived, *up_pieces)
    out = expert_down(own, hidden, *down_pieces)
    returned = lax.all_to_all(
        out.reshape(chips, 2 * CAP, -1), CHIPS, split_axis=0, concat_axis=0, tiled=True
    ).reshape(out.shape)

    y, ys = lax.axis_index("y"), lax.axis_size("y")
    part = jnp.stack([2 * c + v for c in (core, 1 - core) for v in (y % 2, 1 - y % 2)])
    part = part.astype(jnp.int32)
    prepared = shared_prep(
        part,
        common_expert_gate_weight,
        common_expert_up_weight,
        common_expert_down_weight,
    )
    crossed = {}
    for k in (1, 3, 2):
        crossed[k] = lax.ppermute(prepared, "tp", [(i, (i + k) % tp) for i in range(tp)])
    beside = [
        (2 * i + c, 2 * ((i + 1 - 2 * ((i + c) % 2)) % ys) + c) for i in range(ys) for c in range(2)
    ]

    def spread_out(piece):
        pair = [piece, lax.ppermute(piece, ("y", "c"), beside)]
        return pair + [lax.ppermute(v, "c", [(0, 1), (1, 0)]) for v in pair]

    most = spread_out(jnp.concatenate([prepared, crossed[1], crossed[3]], axis=0))
    rest = spread_out(crossed[2])
    shared_sum, columns = shared_expert(
        part, ids_t, routed_expert_weight.T, normed, most, rest
    )
    experts_out = combine(returned, shared_sum, columns, moe_gain.reshape(1, -1))
    return (mixer_out, experts_out)


def solution(mesh):
    split = Mesh(mesh.devices.reshape(8, 4, 2, mesh.shape["tp"]), ("z", "y", "c", "tp"))
    placed = (
        P(EP_TP, None),
        P(EP_TP, None),
        P(EP_TP, None),
        P(),
        P(),
        P(),
        P(EP_TP, None),
        P(),
        P(EP_TP, None),
        P(EP_TP, None),
        P(EP, None, "tp"),
        P(EP, None, "tp"),
        P(EP, "tp", None),
        P(None, "tp"),
        P(None, "tp"),
        P("tp", None),
        P(),
    )
    return jax.shard_map(
        body,
        mesh=split,
        in_specs=placed,
        out_specs=(P(EP_TP, None), P(EP_TP, None)),
        check_vma=False,
    )
```

```python
import math

import jax
import jax.numpy as jnp
from jax import lax
from jax.experimental import pallas as pl
from jax.experimental.pallas import tpu as pltpu
from jax.sharding import Mesh
from jax.sharding import PartitionSpec as P


HEADS = 16
KV_HEADS = 4
HEAD_DIM = 64
WINDOW = 128
CAP = 4
BLOCK = 256
WIDE = 512
MIB = 1 << 20
PARTS = 4
COMBINE_LIMIT = 16
UP_LIMIT = 24
DOWN_LIMIT = 16
EP = ("z", "y", "c")
EP_TP = ("z", "y", "c", "tp")
CHIPS = ("tp", "z", "y")
CORE_TP = ("c", "tp")
EPS = 1e-06
NEGATIVE = -1e30


f32 = jnp.float32
bf16 = jnp.bfloat16
VMEM = pltpu.VMEM
ANY = pl.ANY


def iota(shape, dim):
    return lax.broadcasted_iota(jnp.int32, shape, dim)


def dot(a, b):
    return jnp.dot(a, b, preferred_element_type=f32)


def dot_t(a, b):
    return lax.dot_general(a, b, (((1,), (1,)), ((), ())), preferred_element_type=f32)


def in_vmem(count):
    return [pl.BlockSpec(memory_space=VMEM)] * count


def from_behind(block, axis, distance):
    devices = range(lax.axis_size(axis))
    route = [(i - distance, i) for i in devices if i - distance in devices]
    return lax.ppermute(block, axis, route)


def rms_scale(inputs, gain_vec):
    mean_sq = jnp.mean(inputs * inputs, axis=-1, keepdims=True)
    return inputs * lax.rsqrt(mean_sq + EPS) * gain_vec


def chip_index(ids):
    return (ids & 3) * 32 + (ids >> 4) * 4 + ((ids >> 2) & 3)


def slot_rows(ids, lanes):
    tokens = ids.shape[1]
    shape = (tokens, tokens)
    eye = iota(shape, 0) == iota(shape, 1)
    across = [ids[k : k + 1, :] for k in range(2)]
    down = [jnp.sum(jnp.where(eye, a, 0.0), axis=1, keepdims=True) for a in across]
    if lanes:
        mine, theirs, axis, earlier = across, down, 0, iota(shape, 0) < iota(shape, 1)
    else:
        mine, theirs, axis, earlier = down, across, 1, iota(shape, 1) < iota(shape, 0)
    rows = []
    for k in range(2):
        place = sum(
            jnp.sum(jnp.where((mine[k] == other) & earlier, 1.0, 0.0), axis=axis, keepdims=True)
            for other in theirs
        )
        rows.append((mine[k] * (2 * CAP) + place).astype(jnp.int32))
    return rows


def pack_kernel(
    expert_ref, x_ref, gain_ref, ids_ref, gate_ref, up_ref, packed_ref, normed_ref, piece_ref, *scratch
):
    stacked, made, held, sems, block_sems = scratch
    half = x_ref.shape[1] // 2
    tokens = x_ref.shape[0]
    ins, outs = expert_copies(expert_ref[0], (gate_ref, up_ref), held, piece_ref, sems)
    for c in ins:
        c.start()
    x = x_ref[...].astype(f32)
    normed = rms_scale(x, gain_ref[...]).astype(bf16)
    normed_ref[...] = normed
    stacked[:tokens, :] = normed[:, :half]
    stacked[tokens:, :] = normed[:, half:]
    rows = slot_rows(chip_index(ids_ref[...]).astype(f32), True)
    size = made.shape[0] // block_sems.shape[0]
    blocks = []
    for i in range(block_sems.shape[0]):
        at = pl.ds(i * size, size)
        blocks.append(pltpu.make_async_copy(made.at[at], packed_ref.at[at], block_sems.at[i]))
    for i, block in enumerate(blocks):
        r = iota((size, tokens), 0) + i * size
        chosen = jnp.concatenate(
            [
                jnp.where((r == rows[0] + h * CAP) | (r == rows[1] + h * CAP), 1.0, 0.0).astype(
                    bf16
                )
                for h in range(2)
            ],
            axis=1,
        )
        made[i * size : (i + 1) * size, :] = dot(chosen, stacked[...]).astype(bf16)
        block.start()
        if i == 0:
            for c, d in zip(ins, outs):
                c.wait()
                d.start()
    for c in blocks + outs:
        c.wait()


def pack(expert, x, gain, ids, gate, up, slots):
    tokens, width = x.shape
    rows = gate.shape[1]
    steps = 4
    total = 2 * slots
    hbm = pl.BlockSpec(memory_space=ANY)
    vmem = pl.BlockSpec(memory_space=VMEM)
    return pl.pallas_call(
        pack_kernel,
        in_specs=[pl.BlockSpec(memory_space=pltpu.SMEM), vmem, vmem, vmem, hbm, hbm],
        out_specs=[hbm, vmem, hbm],
        out_shape=[
            jax.ShapeDtypeStruct((total, width // 2), bf16),
            jax.ShapeDtypeStruct((tokens, width), bf16),
            jax.ShapeDtypeStruct((2 * rows, width), bf16),
        ],
        scratch_shapes=[
            VMEM((2 * tokens, width // 2), bf16),
            VMEM((total, width // 2), bf16),
            VMEM((2 * rows, width), bf16),
            pltpu.SemaphoreType.DMA((2, 2)),
            pltpu.SemaphoreType.DMA((steps,)),
        ],
        compiler_params=pltpu.CompilerParams(vmem_limit_bytes=63 * MIB),
        cost_estimate=pl.CostEstimate(
            flops=2 * total * tokens * width, bytes_accessed=6 * tokens * width, transcendentals=0
        ),
        name="pack",
    )(expert, x, gain, ids, gate, up)


def expert_copies(j, arrays, held, out, sems):
    rows = arrays[0].shape[1]
    ins, outs = [], []
    for m, array in enumerate(arrays):
        at = pl.ds(m * rows, rows)
        ins.append(pltpu.make_async_copy(array.at[j], held.at[at], sems.at[0, m]))
        outs.append(pltpu.make_async_copy(held.at[at], out.at[at], sems.at[1, m]))
    return ins, outs


def pick_kernel(expert_ref, *refs):
    ins, outs = expert_copies(expert_ref[0], refs[:-3], refs[-2], refs[-3], refs[-1])
    for c in ins:
        c.start()
    for c, d in zip(ins, outs):
        c.wait()
        d.start()
    for d in outs:
        d.wait()


def pick(expert, arrays, limit):
    rows, width = arrays[0].shape[1:]
    count = len(arrays)
    return pl.pallas_call(
        pick_kernel,
        in_specs=[pl.BlockSpec(memory_space=pltpu.SMEM)] + [pl.BlockSpec(memory_space=ANY)] * count,
        out_specs=pl.BlockSpec(memory_space=ANY),
        out_shape=jax.ShapeDtypeStruct((count * rows, width), bf16),
        scratch_shapes=[VMEM((count * rows, width), bf16), pltpu.SemaphoreType.DMA((2, count))],
        compiler_params=pltpu.CompilerParams(vmem_limit_bytes=limit * MIB),
        cost_estimate=pl.CostEstimate(
            flops=1000, bytes_accessed=4 * count * rows * width, transcendentals=0
        ),
        name="pick",
    )(expert, *arrays)


def start_pieces(own_ref, own, other, copy, parts):
    for mine, pieces in ((1, own), (0, other)):

        @pl.when(own_ref[0] == mine)
        def _():
            for m in range(parts):
                for k, piece in enumerate(pieces):
                    copy(k, m, piece).start()


def up_kernel(own_ref, recv, *refs):
    own, other = refs[:4], refs[4:8]
    hidden_ref, arrived, gate, up, rows, sem, sems = refs[8:]
    part = own[0].shape[0] // 2
    half = recv.shape[1]

    def copy(k, m, piece):
        return pltpu.make_async_copy(
            piece.at[pl.ds(m * part, part)], (gate, up)[m].at[pl.ds(k * part, part)], sems.at[m, k]
        )

    rows_in = pltpu.make_async_copy(recv, arrived, sem)
    rows_in.start()
    start_pieces(own_ref, own, other, copy, 2)
    a, b = iota((BLOCK // 2, BLOCK), 0), iota((BLOCK // 2, BLOCK), 1)
    first = (a // CAP) * (2 * CAP) + a % CAP
    picks = [jnp.where(b == first + h * CAP, 1.0, 0.0).astype(bf16) for h in range(2)]
    rows_in.wait()

    def sort_rows(i, carry):
        block = arrived[pl.ds(pl.multiple_of(i * BLOCK, BLOCK), BLOCK), :]
        at = pl.ds(pl.multiple_of(i * (BLOCK // 2), BLOCK // 2), BLOCK // 2)
        for h in range(2):
            rows[at, h * half : (h + 1) * half] = dot(picks[h], block).astype(bf16)
        return carry

    lax.fori_loop(0, recv.shape[0] // BLOCK, sort_rows, 0)
    for m in range(2):
        for k in range(4):
            copy(k, m, own[k]).wait()

    def units(n, carry):
        at = pl.ds(pl.multiple_of(n * BLOCK, BLOCK), BLOCK)
        x = rows[...]
        g = dot_t(x, gate[at, :])
        u = dot_t(x, up[at, :])
        hidden_ref[:, at] = (g / (1.0 + jnp.exp(-g)) * u).astype(bf16)
        return carry

    lax.fori_loop(0, hidden_ref.shape[1] // BLOCK, units, 0)


def expert_up(own, recv, mine, others):
    total, half = recv.shape
    units = 2 * mine[0].shape[0]
    return pl.pallas_call(
        up_kernel,
        in_specs=[pl.BlockSpec(memory_space=pltpu.SMEM)] + [pl.BlockSpec(memory_space=ANY)] * 9,
        out_specs=pl.BlockSpec(memory_space=VMEM),
        out_shape=jax.ShapeDtypeStruct((total // 2, units), bf16),
        scratch_shapes=[
            VMEM((total, half), bf16),
            VMEM((units, 2 * half), bf16),
            VMEM((units, 2 * half), bf16),
            VMEM((total // 2, 2 * half), bf16),
            pltpu.SemaphoreType.DMA,
            pltpu.SemaphoreType.DMA((2, 4)),
        ],
        compiler_params=pltpu.CompilerParams(vmem_limit_bytes=UP_LIMIT * MIB),
        cost_estimate=pl.CostEstimate(
            flops=4 * total * half * units,
            bytes_accessed=2 * total * half + 8 * half * units,
            transcendentals=total * units // 2,
        ),
        name="expert_up",
    )(own, recv, *mine, *others)


def down_kernel(own_ref, hidden, *refs):
    own, other = refs[:4], refs[4:8]
    out_ref, down, made, sems, out_sems = refs[8:]
    part = own[0].shape[0]
    half = out_ref.shape[1]
    count = half // WIDE

    def copies(n, pieces):
        return [
            pltpu.make_async_copy(
                piece.at[:, pl.ds(h * half + n * WIDE, WIDE)],
                down.at[pl.ds(k * part, part), pl.ds(h * half + n * WIDE, WIDE)],
                sems.at[n, h, k],
            )
            for h in range(2)
            for k, piece in enumerate(pieces)
        ]

    for mine, pieces in ((1, own), (0, other)):

        @pl.when(own_ref[0] == mine)
        def _():
            for n in range(count):
                for c in copies(n, pieces):
                    c.start()

    tiles = hidden.shape[0] // (2 * CAP)
    low = iota((tiles, 2 * CAP, WIDE), 1) < CAP
    for n in range(count):
        for c in copies(n, own):
            c.wait()
        at = n * WIDE
        x = hidden[...]
        left = dot(x, down[:, at : at + WIDE]).reshape(tiles, 2 * CAP, WIDE)
        right = dot(x, down[:, half + at : half + at + WIDE]).reshape(tiles, 2 * CAP, WIDE)
        one = jnp.where(low, left, pltpu.roll(right, CAP, 1))
        two = jnp.where(low, pltpu.roll(left, CAP, 1), right)
        both = jnp.stack([one, two], axis=1).reshape(out_ref.shape[0], WIDE)
        made[:, at : at + WIDE] = both.astype(bf16)
        columns = pl.ds(at, WIDE)
        pltpu.make_async_copy(made.at[:, columns], out_ref.at[:, columns], out_sems.at[n]).start()
    for n in range(count):
        columns = pl.ds(n * WIDE, WIDE)
        pltpu.make_async_copy(made.at[:, columns], out_ref.at[:, columns], out_sems.at[n]).wait()


def expert_down(own, hidden, mine, others):
    rows, units = hidden.shape
    width = mine[0].shape[1]
    count = width // 2 // WIDE
    return pl.pallas_call(
        down_kernel,
        in_specs=[pl.BlockSpec(memory_space=pltpu.SMEM)]
        + in_vmem(1)
        + [pl.BlockSpec(memory_space=ANY)] * 8,
        out_specs=pl.BlockSpec(memory_space=ANY),
        out_shape=jax.ShapeDtypeStruct((2 * rows, width // 2), bf16),
        scratch_shapes=[
            VMEM((units, width), bf16),
            VMEM((2 * rows, width // 2), bf16),
            pltpu.SemaphoreType.DMA((count, 2, 4)),
            pltpu.SemaphoreType.DMA((count,)),
        ],
        compiler_params=pltpu.CompilerParams(vmem_limit_bytes=DOWN_LIMIT * MIB),
        cost_estimate=pl.CostEstimate(
            flops=2 * rows * units * width,
            bytes_accessed=2 * (rows * (units + width) + units * width),
            transcendentals=0,
        ),
        name="expert_down",
    )(own, hidden, *mine, *others)


def shared_prep_kernel(part_ref, gate_ref, up_ref, down_ref, out_ref):
    depth = gate_ref.shape[0] // PARTS
    units = gate_ref.shape[1]
    first = pl.multiple_of(part_ref[0] * depth, depth)
    at = pl.ds(first, depth)
    out_ref[:depth, :] = gate_ref[at, :]
    out_ref[depth : 2 * depth, :] = up_ref[at, :]
    for t in range(depth // 128):
        lane = pl.multiple_of(first + t * 128, 128)
        out_ref[2 * depth + t * units : 2 * depth + (t + 1) * units, :] = down_ref[
            :, pl.ds(lane, 128)
        ]


def shared_prep(part, gate, up, down):
    return pl.pallas_call(
        shared_prep_kernel,
        in_specs=[pl.BlockSpec(memory_space=pltpu.SMEM)] + in_vmem(3),
        out_specs=pl.BlockSpec(memory_space=VMEM),
        out_shape=jax.ShapeDtypeStruct((gate.shape[0] // PARTS * 3, gate.shape[1]), bf16),
        compiler_params=pltpu.CompilerParams(vmem_limit_bytes=8 * MIB),
        cost_estimate=pl.CostEstimate(flops=1000, bytes_accessed=8 * gate.size, transcendentals=0),
        name="shared_prep",
    )(part, gate, up, down)


def slot_columns(ids, weights):
    tokens = ids.shape[1]
    first = slot_rows(chip_index(ids).astype(f32), False)
    eye = iota((tokens, tokens), 0) == iota((tokens, tokens), 1)
    lane = iota((tokens, 128), 1)
    out = jnp.zeros((tokens, 128), f32)
    for k in range(2):
        weight = jnp.sum(jnp.where(eye, weights[k : k + 1, :], 0.0), axis=1, keepdims=True)
        out = jnp.where(lane == k, first[k].astype(f32), out)
        out = jnp.where(lane == 2 + k, weight, out)
    return out


def shared_kernel(part_ref, ids_ref, weight_ref, x_ref, *refs):
    most, last = refs[:PARTS], refs[PARTS : 2 * PARTS]
    out_ref, columns_ref, into, down = refs[2 * PARTS :]
    depth = x_ref.shape[1] // PARTS
    units = most[0].shape[1]
    for p in range(PARTS):
        first = pl.multiple_of(part_ref[p] * depth, depth)
        for k in range(4):
            ref, base = (most[p], 3 * k * depth) if k < 3 else (last[p], 0)
            for m in range(2):
                lane = (m * 4 + k) * units
                into[pl.ds(first, depth), lane : lane + units] = ref[
                    base + m * depth : base + (m + 1) * depth, :
                ]
            for t in range(depth // 128):
                lane = pl.multiple_of(first + t * 128, 128)
                at = base + 2 * depth + t * units
                down[k * units : (k + 1) * units, pl.ds(lane, 128)] = ref[at : at + units, :]
    both = dot(x_ref[...], into[...])
    g, u = both[:, : 4 * units], both[:, 4 * units :]
    hidden = (g / (1.0 + jnp.exp(-g)) * u).astype(bf16)
    out_ref[...] = dot(hidden, down[...])
    columns_ref[...] = slot_columns(ids_ref[...], weight_ref[...])


def shared_expert(part, ids, weights, normed, most, last):
    tokens, width = normed.shape
    units = 4 * most[0].shape[1]
    return pl.pallas_call(
        shared_kernel,
        in_specs=[pl.BlockSpec(memory_space=pltpu.SMEM)] + in_vmem(3 + 2 * PARTS),
        out_specs=[pl.BlockSpec(memory_space=VMEM)] * 2,
        out_shape=[
            jax.ShapeDtypeStruct((tokens, width), f32),
            jax.ShapeDtypeStruct((tokens, 128), f32),
        ],
        scratch_shapes=[VMEM((width, 2 * units), bf16), VMEM((units, width), bf16)],
        compiler_params=pltpu.CompilerParams(vmem_limit_bytes=24 * MIB),
        cost_estimate=pl.CostEstimate(
            flops=6 * tokens * width * units,
            bytes_accessed=6 * width * units,
            transcendentals=tokens * units,
        ),
        name="shared_expert",
    )(part, ids, weights, normed, *most, *last)


def combine_kernel(back_ref, shared_ref, columns_ref, gain_ref, out_ref):
    tokens, half = out_ref.shape[0], back_ref.shape[1]
    r = iota((tokens, back_ref.shape[0]), 1)
    first = [columns_ref[:, k : k + 1].astype(jnp.int32) for k in range(2)]
    weights = [columns_ref[:, 2 + k : 3 + k] for k in range(2)]
    spreads = []
    for h in range(2):
        spread = jnp.where(r == first[0] + h * CAP, weights[0], 0.0) + jnp.where(
            r == first[1] + h * CAP, weights[1], 0.0
        )
        spreads.append(spread.astype(bf16))
    spread = jnp.concatenate(spreads, axis=0)
    summed = dot(spread, back_ref[...])
    halves = [
        summed[h * tokens : (h + 1) * tokens] + shared_ref[:, h * half : (h + 1) * half]
        for h in range(2)
    ]
    square = sum(jnp.sum(v * v, axis=1, keepdims=True) for v in halves)
    scale = lax.rsqrt(square / (2 * half) + EPS)
    for h, v in enumerate(halves):
        at = slice(h * half, (h + 1) * half)
        out_ref[:, at] = (v * scale * gain_ref[:, at]).astype(bf16)


def combine(back, shared, columns, gain):
    slots, half = back.shape
    tokens = shared.shape[0]
    return pl.pallas_call(
        combine_kernel,
        in_specs=in_vmem(4),
        out_specs=pl.BlockSpec(memory_space=VMEM),
        out_shape=jax.ShapeDtypeStruct((tokens, 2 * half), bf16),
        compiler_params=pltpu.CompilerParams(vmem_limit_bytes=COMBINE_LIMIT * MIB),
        cost_estimate=pl.CostEstimate(
            flops=8 * tokens * slots * half, bytes_accessed=2 * slots * half, transcendentals=0
        ),
        name="combine",
    )(back, shared, columns, gain)


def attention_kernel(
    first_ref, sink_ref, q_ref, k_ref, v_ref, rim_ref, weight_ref, gain_ref, out_ref, keys, values, mix, wide
):
    tokens = q_ref.shape[0]
    lanes = 2 * HEAD_DIM
    group = HEADS // KV_HEADS
    tiles = k_ref.shape[1] // lanes
    for into, rim, own in ((keys, 0, k_ref), (values, 1, v_ref)):
        for t in range(tiles):
            at = slice(t * lanes, (t + 1) * lanes)
            rows = jnp.concatenate([rim_ref[rim, :, at], own[:, at]], axis=0)
            into[2 * t] = rows
            into[2 * t + 1] = jnp.concatenate([rows[:, HEAD_DIM:], rows[:, :HEAD_DIM]], axis=1)
    i, j = iota((WINDOW, 2 * WINDOW), 0), iota((WINDOW, 2 * WINDOW), 1)
    low = iota((WINDOW, lanes), 1) < HEAD_DIM

    for n in range(tokens // WINDOW):
        band = slice(n * WINDOW, (n + 2) * WINDOW)
        at = slice(n * WINDOW, (n + 1) * WINDOW)
        inside = (j > i) & (j <= i + WINDOW)
        if n == 0:
            inside = inside & (j >= first_ref[0] * WINDOW)
        for g in range(KV_HEADS):
            kt = [2 * (g // 2) + (g + s) % 2 for s in range(2)]
            for t in range(group // 2):
                tile = g * (group // 2) + t
                q = q_ref[at, tile * lanes : (tile + 1) * lanes]
                mixed = []
                for s in range(2):
                    mine = jnp.where(low if s == 0 else ~low, q, jnp.zeros_like(q))
                    score = dot_t(mine, keys[kt[s], band, :]) * (1.0 / math.sqrt(HEAD_DIM))
                    score = jnp.where(inside, score, NEGATIVE)
                    sink = sink_ref[2 * tile + s]
                    top = jnp.maximum(jnp.max(score, axis=1, keepdims=True), sink)
                    e = jnp.exp(score - top)
                    below = jnp.sum(e, axis=1, keepdims=True) + jnp.exp(sink - top)
                    mixed.append(dot((e / below).astype(bf16), values[kt[s], band, :]))
                mix[at, tile * lanes : (tile + 1) * lanes] = jnp.where(
                    low, mixed[0], mixed[1]
                ).astype(bf16)

    width = 512
    square = jnp.zeros((tokens, 1), f32)
    for n in range(out_ref.shape[1] // width):
        at = slice(n * width, (n + 1) * width)
        p = dot(mix[...], weight_ref[:, at])
        wide[:, at] = p
        square = square + jnp.sum(p * p, axis=1, keepdims=True)
    scale = lax.rsqrt(square / out_ref.shape[1] + EPS)
    for n in range(out_ref.shape[1] // width):
        at = slice(n * width, (n + 1) * width)
        out_ref[:, at] = (wide[:, at] * scale * gain_ref[:, at]).astype(bf16)


def attention(first, sinks, queries, keys, values, rim, weight, gain):
    tokens, wide = queries.shape[0], weight.shape[1]
    lanes = 2 * HEAD_DIM
    rows = tokens + WINDOW
    return pl.pallas_call(
        attention_kernel,
        in_specs=[pl.BlockSpec(memory_space=pltpu.SMEM)] * 2 + in_vmem(6),
        out_specs=pl.BlockSpec(memory_space=VMEM),
        out_shape=jax.ShapeDtypeStruct((tokens, wide), bf16),
        scratch_shapes=[
            VMEM((KV_HEADS, rows, lanes), bf16),
            VMEM((KV_HEADS, rows, lanes), bf16),
            VMEM((tokens, HEADS * HEAD_DIM), bf16),
            VMEM((tokens, wide), f32),
        ],
        cost_estimate=pl.CostEstimate(
            flops=2 * tokens * HEADS * HEAD_DIM * (wide + 8 * WINDOW),
            bytes_accessed=2 * weight.size + 4 * tokens * wide,
            transcendentals=tokens * HEADS * 2 * WINDOW,
        ),
        compiler_params=pltpu.CompilerParams(vmem_limit_bytes=24 * MIB),
        name="attention",
    )(first, sinks, queries, keys, values, rim, weight, gain)


def body(
    att_queries,
    att_keys,
    att_values,
    sink_logits,
    out_weight,
    att_gain,
    moe_in,
    pre_gain,
    expert_ids,
    routed_expert_weight,
    w_gate,
    w_up,
    w_down,
    common_expert_gate_weight,
    common_expert_up_weight,
    common_expert_down_weight,
    moe_gain,
):
    x, core = lax.axis_index("tp"), lax.axis_index("c")
    tp = lax.axis_size("tp")
    near, far = [], []
    for i in range(tp):
        c = i // 2
        near += [(c * tp + (i - 1) % tp, c * tp + i), (c * tp + (i + 1) % tp, (1 - c) * tp + i)]
        far += [(c * tp + (i + 2) % tp, c * tp + i), (c * tp + i, (1 - c) * tp + i)]
    swapped = [(i, (i + tp) % (2 * tp)) for i in range(2 * tp)]
    own = (core == x // 2).astype(jnp.int32).reshape(1)

    kv_rows = jnp.stack([att_keys, att_values])
    rim_rows = from_behind(kv_rows[:, att_keys.shape[0] - WINDOW :], EP_TP, 1)
    first = (lax.axis_index(EP_TP) == 0).astype(jnp.int32).reshape(1)

    gate_t, up_t = w_gate.transpose(0, 2, 1), w_up.transpose(0, 2, 1)

    even_expert = (x % 2).astype(jnp.int32).reshape(1)
    odd_expert = 1 - even_expert

    def moved(piece, route):
        return lax.ppermute(piece, CORE_TP, route)

    def gathered(came_near, came_far, other_near, other_far):
        return (other_far, came_near, came_far, other_near), (
            came_far,
            other_near,
            other_far,
            came_near,
        )

    near_in = moved(pick(odd_expert, (gate_t, up_t), 63), near)
    ids_t = expert_ids.T
    packed, normed, even = pack(
        even_expert, moe_in, pre_gain.reshape(1, -1), ids_t, gate_t, up_t, 128 * CAP
    )
    far_in = moved(even, far)
    chips = packed.shape[0] // (2 * CAP)
    arrived = lax.all_to_all(
        packed.reshape(chips, 2 * CAP, -1), CHIPS, split_axis=0, concat_axis=0, tiled=True
    ).reshape(packed.shape)

    near_out = moved(pick(odd_expert, (w_down,), 8), near)
    far_out = moved(pick(even_expert, (w_down,), 8), far)
    up_pieces = gathered(near_in, far_in, moved(near_in, swapped), moved(far_in, swapped))
    down_pieces = gathered(near_out, far_out, moved(near_out, swapped), moved(far_out, swapped))

    mixer_out = attention(
        first,
        sink_logits,
        att_queries,
        att_keys,
        att_values,
        rim_rows,
        out_weight,
        att_gain.reshape(1, -1),
    )

    hidden = expert_up(own, arrived, *up_pieces)
    out = expert_down(own, hidden, *down_pieces)
    returned = lax.all_to_all(
        out.reshape(chips, 2 * CAP, -1), CHIPS, split_axis=0, concat_axis=0, tiled=True
    ).reshape(out.shape)

    y, ys = lax.axis_index("y"), lax.axis_size("y")
    part = jnp.stack([2 * c + v for c in (core, 1 - core) for v in (y % 2, 1 - y % 2)])
    part = part.astype(jnp.int32)
    prepared = shared_prep(
        part,
        common_expert_gate_weight,
        common_expert_up_weight,
        common_expert_down_weight,
    )
    crossed = {}
    for k in (1, 3, 2):
        crossed[k] = lax.ppermute(prepared, "tp", [(i, (i + k) % tp) for i in range(tp)])
    beside = [
        (2 * i + c, 2 * ((i + 1 - 2 * ((i + c) % 2)) % ys) + c) for i in range(ys) for c in range(2)
    ]

    def spread_out(piece):
        pair = [piece, lax.ppermute(piece, ("y", "c"), beside)]
        return pair + [lax.ppermute(v, "c", [(0, 1), (1, 0)]) for v in pair]

    most = spread_out(jnp.concatenate([prepared, crossed[1], crossed[3]], axis=0))
    rest = spread_out(crossed[2])
    shared_sum, columns = shared_expert(
        part, ids_t, routed_expert_weight.T, normed, most, rest
    )
    experts_out = combine(returned, shared_sum, columns, moe_gain.reshape(1, -1))
    return (mixer_out, experts_out)


def solution(mesh):
    split = Mesh(mesh.devices.reshape(8, 4, 2, mesh.shape["tp"]), ("z", "y", "c", "tp"))
    placed = (
        P(EP_TP, None),
        P(EP_TP, None),
        P(EP_TP, None),
        P(),
        P(),
        P(),
        P(EP_TP, None),
        P(),
        P(EP_TP, None),
        P(EP_TP, None),
        P(EP, None, "tp"),
        P(EP, None, "tp"),
        P(EP, "tp", None),
        P(None, "tp"),
        P(None, "tp"),
        P("tp", None),
        P(),
    )
    return jax.shard_map(
        body,
        mesh=split,
        in_specs=placed,
        out_specs=(P(EP_TP, None), P(EP_TP, None)),
        check_vma=False,
    )
```
